32 devices in a mesh: sp: 16 (over z, y, x), tp: 2 (over core).
Axes of the slice: x: 2, y: 2, z: 4, core: 2. Of those that a mesh axis runs over, the one named last changes fastest.
Arguments:
- residual: bfloat16 [2048, 2048], P(('sp', 'tp')), may hold values from -24 to 24
- query_small: bfloat16 [2048, 768], P('sp', 'tp'), may hold values from -64 to 64
- query_large: bfloat16 [2048, 1280], P('sp', 'tp'), may hold values from -64 to 64
- latent: bfloat16 [2048, 256], P('sp'), may hold values from -6 to 6
- rope_key: bfloat16 [2048, 32], P('sp'), may hold values from -48 to 48
- key_up_small: bfloat16 [256, 512], P(None, 'tp'), may hold values from -0.375 to 0.375
- value_up_small: bfloat16 [256, 512], P(None, 'tp'), may hold values from -0.375 to 0.375
- key_up_large: bfloat16 [256, 1024], P(None, 'tp'), may hold values from -0.375 to 0.375
- value_up_large: bfloat16 [256, 1024], P(None, 'tp'), may hold values from -0.375 to 0.375
- out_small: bfloat16 [512, 2048], P('tp'), may hold values from -0.625 to 0.625
- out_large: bfloat16 [1024, 2048], P('tp'), may hold values from -0.625 to 0.625
- norm_gain: bfloat16 [2048], replicated, may hold values from 0.099609375 to 1.8984375
- gate_weight: bfloat16 [2048, 5632], P('sp', 'tp'), may hold values from -0.125 to 0.125
- up_weight: bfloat16 [2048, 5632], P('sp', 'tp'), may hold values from -0.125 to 0.125
- down_weight: bfloat16 [2048, 5632], P('sp', 'tp'), may hold values from -0.21875 to 0.21875
Outputs:
- layer_out: bfloat16 [2048, 2048], P(('sp', 'tp'))
The draws below stay inside these ranges and needn't reach their ends.
All inputs are finite; a program needn't handle non-finite values.
Results may differ from the reference program's by a relative error of at most 0.017.
Values may be sent and summed in bfloat16 or wider, within the bound.
A program may use at most 128 MiB of HBM per device.

```python
import jax
import jax.numpy as jnp
from jax import lax

D = 2048
FF = 5632
HEADS_SMALL = 8
HEADS_LARGE = 8
HEAD_SMALL = 64
HEAD_LARGE = 128
ROPE = 32
LATENT = 256
TOKENS = 2048


def draw_residual(key, part):
    subkeys = jax.random.split(key, 3)
    lowest = 0.3
    highest = 3.0
    column = jnp.exp(jax.random.uniform(subkeys[0], (1, D), jnp.float32, jnp.log(lowest), jnp.log(highest)))
    rowscale = jnp.exp(jax.random.uniform(subkeys[1], (TOKENS, 1), jnp.float32, jnp.log(0.5), jnp.log(2.0)))
    sample = jnp.clip(jax.random.normal(subkeys[2], (TOKENS, D), jnp.float32), -4.0, 4.0)
    return jnp.clip(sample * rowscale * column, -24.0, 24.0).astype(jnp.bfloat16)


def drawn_query(key, head_count, head_size):
    span_width = head_size + ROPE
    sample = jnp.clip(2.5 * jax.random.normal(key, (TOKENS, head_count, span_width), jnp.float32), -10.0, 10.0)
    return sample.reshape(TOKENS, head_count * span_width).astype(jnp.bfloat16)


def draw_query_small(key, part):
    return drawn_query(jax.random.fold_in(key, 11), HEADS_SMALL, HEAD_SMALL)


def draw_query_large(key, part):
    return drawn_query(jax.random.fold_in(key, 23), HEADS_LARGE, HEAD_LARGE)


def draw_rope_key(key, part):
    sample = jnp.clip(jax.random.normal(key, (TOKENS, ROPE), jnp.float32), -6.0, 6.0)
    return sample.astype(jnp.bfloat16)


def steps_of(rng, dims, cuts, least, largest):
    def one(position, blocks):
        steps = jax.random.uniform(jax.random.fold_in(jax.random.fold_in(rng, 6), position), (blocks,), jnp.float32, least / len(cuts), largest / len(cuts))
        return jnp.repeat(jnp.exp(steps), dims[position] // blocks).reshape((-1,) + (1,) * (len(dims) - position - 1))

    loudness = one(*cuts[0])
    for cut in cuts[1:]:
        loudness = loudness * one(*cut)
    return loudness


def bell_draw(own_key, shape, spread, reach, shards=(), kind=jnp.bfloat16):
    gain = steps_of(own_key, shape, shards, -0.22, 0.18) if shards else 1.0
    drawn = jax.random.normal(own_key, shape, jnp.float32) * spread * gain
    return jnp.minimum(jnp.maximum(drawn, -reach), reach).astype(kind)


def setup_inputs(seed: int = 0) -> dict:
    seeds = jax.random.split(jax.random.key(seed), 16)
    residual = draw_residual(jax.random.fold_in(seeds[15], 71), 0)
    query_small = draw_query_small(jax.random.fold_in(seeds[15], 71), 0)
    query_large = draw_query_large(jax.random.fold_in(seeds[15], 71), 0)
    latent = bell_draw(seeds[3], (TOKENS, LATENT), 1.0, 6.0, ((0, 16),))
    rope_key = draw_rope_key(jax.random.fold_in(seeds[15], 71), 0)
    key_up_small = bell_draw(seeds[5], (LATENT, HEADS_SMALL * HEAD_SMALL), LATENT ** -0.5, 0.375, ((1, 2),))
    value_up_small = bell_draw(seeds[6], (LATENT, HEADS_SMALL * HEAD_SMALL), LATENT ** -0.5, 0.375, ((1, 2),))
    key_up_large = bell_draw(seeds[7], (LATENT, HEADS_LARGE * HEAD_LARGE), LATENT ** -0.5, 0.375, ((1, 2),))
    value_up_large = bell_draw(seeds[8], (LATENT, HEADS_LARGE * HEAD_LARGE), LATENT ** -0.5, 0.375, ((1, 2),))
    out_small = bell_draw(seeds[9], (HEADS_SMALL * HEAD_SMALL, D), ((HEADS_SMALL * HEAD_SMALL + HEADS_LARGE * HEAD_LARGE) // 16) ** -0.5, 0.625, ((0, 2),))
    out_large = bell_draw(seeds[10], (HEADS_LARGE * HEAD_LARGE, D), ((HEADS_SMALL * HEAD_SMALL + HEADS_LARGE * HEAD_LARGE) // 16) ** -0.5, 0.625, ((0, 2),))
    norm_gain = jnp.clip(1.0 + 0.18 * jax.random.normal(seeds[11], (D,), jnp.float32), 0.099609375, 1.8984375).astype(jnp.bfloat16)
    gate_weight = bell_draw(seeds[12], (D, FF), D ** -0.5, 0.125, ((0, 16), (1, 2)))
    up_weight = bell_draw(seeds[13], (D, FF), D ** -0.5, 0.125, ((0, 16), (1, 2)))
    down_weight = bell_draw(seeds[14], (D, FF), (FF // 8) ** -0.5, 0.21875, ((0, 16), (1, 2)))
    return {"residual": residual, "query_small": query_small, "query_large": query_large, "latent": latent, "rope_key": rope_key, "key_up_small": key_up_small, "value_up_small": value_up_small, "key_up_large": key_up_large, "value_up_large": value_up_large, "out_small": out_small, "out_large": out_large, "norm_gain": norm_gain, "gate_weight": gate_weight, "up_weight": up_weight, "down_weight": down_weight}


big_negative = -1e+30
rope_base = 500000.0
norm_eps = 1e-06

def stored(tensor):
    return lax.optimization_barrier(tensor.astype(jnp.bfloat16))

def rotate_stored(vectors, positions):
    span_width = vectors.shape[-1]
    half_width = span_width // 2
    inverse = 1.0 / rope_base ** (jnp.arange(0, span_width, 2, dtype=jnp.float32) / span_width)
    angles = positions.astype(jnp.float32)[:, None] * inverse[None, :]
    angle_shape = (vectors.shape[0],) + (1,) * (vectors.ndim - 2) + (half_width,)
    cosine = jnp.cos(angles).reshape(angle_shape)
    sine_table = jnp.sin(angles).reshape(angle_shape)
    leading = vectors[..., :half_width].astype(jnp.float32)
    trailing = vectors[..., half_width:].astype(jnp.float32)
    turned = jnp.concatenate([leading * cosine - trailing * sine_table, trailing * cosine + leading * sine_table], axis=-1)
    return stored(turned)

def attend_group(query, latent, key_up, value_up, turned_key, positions, head_count, head_size):
    shaped = query.reshape(TOKENS, head_count, head_size + ROPE)
    nope_part = shaped[..., :head_size]
    turned_query = rotate_stored(shaped[..., head_size:], positions)
    key_rows = stored(jnp.dot(latent, key_up, preferred_element_type=jnp.float32)).reshape(TOKENS, head_count, head_size)
    value_rows = stored(jnp.dot(latent, value_up, preferred_element_type=jnp.float32)).reshape(TOKENS, head_count, head_size)
    scale = (head_size + ROPE) ** (-0.5)
    block_rows = min(256, TOKENS)

    def one_block(block_index):
        offset = block_index * block_rows
        query_nope = lax.dynamic_slice_in_dim(nope_part, offset, block_rows, 0).astype(jnp.float32)
        query_turn = lax.dynamic_slice_in_dim(turned_query, offset, block_rows, 0).astype(jnp.float32)
        query_pos = offset + jnp.arange(block_rows, dtype=jnp.int32)
        scores = jnp.einsum('qhe,khe->qhk', query_nope, key_rows.astype(jnp.float32))
        scores = scores + jnp.einsum('qhr,kr->qhk', query_turn, turned_key.astype(jnp.float32))
        scores = scores * scale
        visible = positions[None, None, :] <= query_pos[:, None, None]
        masked = jnp.where(visible, scores, big_negative)
        maxima = lax.optimization_barrier(jnp.max(masked, axis=2, keepdims=True))
        weights = jnp.where(visible, jnp.exp(masked - maxima), 0.0)
        totals = lax.optimization_barrier(jnp.sum(weights, axis=2))
        rounded = stored(weights).astype(jnp.float32)
        result = jnp.einsum('qhk,khe->qhe', rounded, value_rows.astype(jnp.float32)) / totals[:, :, None]
        return result.reshape(block_rows, head_count * head_size).astype(jnp.bfloat16)
    blocks = lax.map(one_block, jnp.arange(TOKENS // block_rows, dtype=jnp.int32))
    return blocks.reshape(TOKENS, head_count * head_size)

def reference(residual, query_small, query_large, latent, rope_key, key_up_small, value_up_small, key_up_large, value_up_large, out_small, out_large, norm_gain, gate_weight, up_weight, down_weight):
    positions = jnp.arange(TOKENS, dtype=jnp.int32)
    turned_key = rotate_stored(rope_key, positions)
    attended_small = attend_group(query_small, latent, key_up_small, value_up_small, turned_key, positions, HEADS_SMALL, HEAD_SMALL)
    attended_large = attend_group(query_large, latent, key_up_large, value_up_large, turned_key, positions, HEADS_LARGE, HEAD_LARGE)
    mixed = jnp.dot(attended_small, out_small, preferred_element_type=jnp.float32)
    mixed = mixed + jnp.dot(attended_large, out_large, preferred_element_type=jnp.float32)
    mixed = stored(mixed)
    stream = stored(residual.astype(jnp.float32) + mixed.astype(jnp.float32))
    as_float = stream.astype(jnp.float32)
    normed = as_float * lax.rsqrt(lax.optimization_barrier(jnp.mean(as_float * as_float, axis=-1, keepdims=True)) + norm_eps)
    normed = (normed * norm_gain.astype(jnp.float32)[None, :]).astype(jnp.bfloat16)
    gate = jnp.dot(normed, gate_weight, preferred_element_type=jnp.float32)
    up_part = jnp.dot(normed, up_weight, preferred_element_type=jnp.float32)
    hidden = (jax.nn.silu(gate) * up_part).astype(jnp.bfloat16)
    channel = lax.dot_general(hidden, down_weight, (((1,), (1,)), ((), ())), preferred_element_type=jnp.float32)
    channel = stored(channel)
    return (as_float + 0.5 * channel.astype(jnp.float32)).astype(jnp.bfloat16)
```

```python
import functools
import math

import jax
import jax.numpy as jnp
from jax import lax
from jax.experimental import pallas as pl
from jax.experimental.pallas import tpu as pltpu
from jax.sharding import PartitionSpec as P

MESH = pl.DeviceIdType.MESH
HEAD_SMALL = 64
HEAD_LARGE = 128
ROPE = 32
LANES = 128


big_negative = -1e30
rope_base = 500000.0
norm_eps = 1e-06


def rotate(vectors, positions):
    span_width = vectors.shape[-1]
    half_width = span_width // 2
    inverse = 1.0 / rope_base ** (jnp.arange(0, span_width, 2, dtype=jnp.float32) / span_width)
    angles = positions.astype(jnp.float32)[:, None] * inverse[None, :]
    angle_shape = (vectors.shape[0],) + (1,) * (vectors.ndim - 2) + (half_width,)
    cosine = jnp.cos(angles).reshape(angle_shape)
    sine_table = jnp.sin(angles).reshape(angle_shape)
    leading = vectors[..., :half_width].astype(jnp.float32)
    trailing = vectors[..., half_width:].astype(jnp.float32)
    turned = jnp.concatenate(
        [leading * cosine - trailing * sine_table, trailing * cosine + leading * sine_table],
        axis=-1,
    )
    return turned.astype(jnp.bfloat16)


def attend(nope_part, turned_query, key_rows, value_rows, turned_key, visible, head_size):
    head_count, row_count = nope_part.shape[:2]
    key_count = key_rows.shape[0]
    key_rows = key_rows.reshape(key_count, head_count, head_size)
    value_rows = value_rows.reshape(key_count, head_count, head_size)
    scores = jnp.einsum("hqe,khe->hqk", nope_part, key_rows, preferred_element_type=jnp.float32)
    scores = scores + jnp.einsum(
        "hqr,kr->hqk", turned_query, turned_key, preferred_element_type=jnp.float32
    )
    scores = scores * (head_size + ROPE) ** (-0.5)
    masked = jnp.where(visible[None, :, :], scores, big_negative)
    maxima = jnp.max(masked, axis=2)
    weights = jnp.where(visible[None, :, :], jnp.exp(masked - maxima[:, :, None]), 0.0)
    totals = jnp.sum(weights, axis=2)
    summed = jnp.einsum(
        "hqk,khe->hqe", weights.astype(jnp.bfloat16), value_rows, preferred_element_type=jnp.float32
    )
    result = summed / totals[:, :, None]
    return (
        jnp.transpose(result, (1, 0, 2))
        .reshape(row_count, head_count * head_size)
        .astype(jnp.bfloat16)
    )


def flip(index, mask):
    bit = 1
    while bit <= mask:
        if mask & bit:
            index = index + bit * (1 - 2 * lax.rem(lax.div(index, bit), 2))
        bit *= 2
    return index


def aligned(index, size):
    return pl.multiple_of(index * size, size)


def mixer(
    plan,
    normed,
    stream,
    gate,
    up,
    down,
    out,
    gate_all,
    up_all,
    down_all,
    rows_all,
    gate_sum,
    up_sum,
    hidden,
    part,
    other,
    summed,
    arrived,
    own_sum,
    copy_sem,
    far_send,
    near_send,
    weight_recv,
    rows_send,
    rows_recv,
    pair_send,
    pair_recv,
    part_send,
    part_recv,
    sum_send,
    sum_recv,
):
    far, near, tp_count, depth, tiles, wide, width = plan
    own_rows = normed.shape[0]
    near_bits = near.bit_length() - 1
    chunk = near * depth
    row_total = far * tp_count * own_rows
    sp_index = lax.axis_index("sp")
    tp_index = lax.axis_index("tp")
    far_index = lax.div(sp_index, near)
    near_index = lax.rem(sp_index, near)

    def place(far_to, near_to, tp_to):
        return {"sp": far_to * near + near_to, "tp": tp_to}

    def first_tile(far_to):
        return lax.div(far_to * tiles + lax.rem(tp_index, 2) * (far - 1), far)

    def tile_count(far_to):
        return first_tile(far_to + 1) - first_tile(far_to)

    def by_count(count, act):
        if tiles % far == 0:
            act(wide)
            return
        for number in (wide - 1, wide):
            if number:
                pl.when(count == number)(functools.partial(act, number))

    inputs = (gate, up, down)
    held = (gate_all, up_all, down_all)
    own_count = tile_count(far_index)

    def source(matrix, far_to, number):
        start = aligned(first_tile(far_to), LANES)
        return inputs[matrix].at[:, pl.ds(start, number * LANES)]

    def block(matrix, far_from, near_from, number):
        start = aligned(far_from * near + near_from, depth)
        return held[matrix].at[pl.ds(start, depth), pl.ds(0, number * LANES)]

    def remote(src, dst, send, recv, device):
        return pltpu.make_async_remote_copy(
            src_ref=src,
            dst_ref=dst,
            send_sem=send,
            recv_sem=recv,
            device_id=device,
            device_id_type=MESH,
        )

    def own_copy(matrix, number):
        return pltpu.make_async_copy(
            source(matrix, far_index, number),
            block(matrix, far_index, near_index, number),
            copy_sem.at[matrix],
        )

    def far_copy(matrix, step, number):
        far_to = flip(far_index, step)
        return remote(
            source(matrix, far_to, number),
            block(matrix, far_index, near_index, number),
            far_send.at[matrix, step],
            weight_recv.at[matrix, step, 0],
            place(far_to, near_index, tp_index),
        )

    def near_order(step):
        return [(step + number) % near_bits for number in range(near_bits)]

    def near_sends(step):
        order = near_order(step)
        sends = []
        for role in range(near):
            reached = max([order.index(b) for b in range(near_bits) if role >> b & 1], default=-1)
            for bit in order[reached + 1 :]:
                sends.append((role, bit))
        return sends

    def near_copy(matrix, step, role, bit, number):
        far_from = flip(far_index, step)
        near_from = flip(near_index, role)
        target = block(matrix, far_from, near_from, number)
        direct = step == 0 and role == 0
        return remote(
            source(matrix, far_index, number) if direct else target,
            target,
            near_send.at[matrix, step, near_sends(step).index((role, bit))],
            weight_recv.at[matrix, step, role | 1 << bit],
            place(far_index, flip(near_index, 1 << bit), tp_index),
        )

    def start_far(matrix, step):
        by_count(
            tile_count(flip(far_index, step)),
            lambda number: far_copy(matrix, step, number).start(),
        )

    def forward(matrix, step, role):
        def act(number):
            for sender, bit in near_sends(step):
                if sender == role:
                    near_copy(matrix, step, role, bit, number).start()

        by_count(own_count, act)

    def await_block(matrix, step, role):
        def act(number):
            if role == 0 and step == 0:
                own_copy(matrix, number).wait()
            else:
                far_from, near_from = flip(far_index, step), flip(near_index, role)
                target = block(matrix, far_from, near_from, number)
                remote(
                    target,
                    target,
                    copy_sem.at[matrix],
                    weight_recv.at[matrix, step, role],
                    place(far_index, flip(near_index, 1), tp_index),
                ).wait_recv()

        by_count(own_count, act)

    relays = [role for role in range(1, near) if any(s == role for s, _ in near_sends(0))]

    def relay_roles(step):
        return sorted({role for role, _ in near_sends(step) if role})

    done = set()

    def take(matrices, step, role):
        for matrix in matrices:
            if (matrix, step, role) not in done:
                done.add((matrix, step, role))
                await_block(matrix, step, role)
                if not (step == 0 and role == 0):
                    forward(matrix, step, role)

    def take_group(matrices, step):
        for role in range(near):
            take(matrices, step, role)

    if tiles % far:
        spare = pl.ds((wide - 1) * LANES, LANES)

        @pl.when(own_count < wide)
        def _():
            gate_all[:, spare] = jnp.zeros((far * chunk, LANES), gate_all.dtype)
            up_all[:, spare] = jnp.zeros((far * chunk, LANES), up_all.dtype)
            down_all[:, spare] = jnp.zeros((far * chunk, LANES), down_all.dtype)

    barrier = pltpu.get_barrier_semaphore()
    peers = [place(flip(far_index, step), near_index, tp_index) for step in range(1, far)]
    peers += [place(far_index, flip(near_index, 1 << b), tp_index) for b in range(near_bits)]
    peers += [place(far_index, near_index, flip(tp_index, j)) for j in range(1, tp_count)]
    for peer in peers:
        pl.semaphore_signal(barrier, inc=1, device_id=peer, device_id_type=MESH)
    pl.semaphore_wait(barrier, len(peers))

    pairs = (0, 1)
    for step in range(1, far):
        for matrix in pairs:
            start_far(matrix, step)
    for matrix in pairs:
        forward(matrix, 0, 0)
    for matrix in range(3):
        by_count(own_count, lambda number: own_copy(matrix, number).start())

    def rows_copy(step):
        return remote(
            normed,
            rows_all.at[far_index, tp_index],
            rows_send.at[step],
            rows_recv.at[step],
            place(flip(far_index, step), near_index, tp_index),
        )

    def pair_copy(step, other_tp):
        far_from = flip(far_index, step)
        target = rows_all.at[far_from, tp_index]
        return remote(
            normed if step == 0 else target,
            target,
            pair_send.at[step, other_tp - 1],
            pair_recv.at[step, other_tp - 1],
            place(far_index, near_index, flip(tp_index, other_tp)),
        )

    for step in range(1, far):
        rows_copy(step).start()
    for other_tp in range(1, tp_count):
        pair_copy(0, other_tp).start()
    rows_all[far_index, tp_index] = normed[...]

    for step in range(1, far):
        start_far(2, step)

    for step in range(1, far):
        take(pairs, step, 0)
        for role in relay_roles(step - 1):
            take(pairs, step - 1, role)
    for role in relay_roles(far - 1):
        take(pairs, far - 1, role)
    forward(2, 0, 0)
    for step in range(1, far):
        rows_copy(step).wait_recv()
        for other_tp in range(1, tp_count):
            pair_copy(step, other_tp).start()
    for step in range(far):
        for other_tp in range(1, tp_count):
            pair_copy(step, other_tp).wait_recv()

    tile = 2 * LANES if width % (2 * LANES) == 0 else LANES
    for step in range(far):
        take_group(pairs, step)
        if step == far - 1:
            take((2,), 1, 0)
        start = aligned(flip(far_index, step), chunk)
        rows = rows_all[:, :, :, pl.ds(start, chunk)].reshape(row_total, chunk)
        for first in range(0, width, tile):
            span = pl.ds(first, tile)
            for weight, total in ((gate_all, gate_sum), (up_all, up_sum)):
                product = jnp.dot(
                    rows, weight[pl.ds(start, chunk), span], preferred_element_type=jnp.float32
                )
                total[:, span] = product if step == 0 else total[:, span] + product
    for first in range(0, width, LANES):
        span = pl.ds(first, LANES)
        value = gate_sum[:, span]
        value = (value / (1.0 + jnp.exp(-value)) * up_sum[:, span]).astype(hidden.dtype)
        if first >= (wide - 1) * LANES and tiles % far:
            value = jnp.where(own_count == wide, value, jnp.zeros_like(value))
        hidden[:, span] = value

    def part_copy(step, other_tp):
        tp_to = flip(tp_index, other_tp)
        return remote(
            part.at[step, :, tp_to],
            other.at[step, other_tp - 1],
            part_send.at[step, other_tp - 1],
            part_recv.at[step, other_tp - 1],
            place(far_index, near_index, tp_to),
        )

    def sum_copy(step, apart):
        far_to = flip(far_index, apart)
        return remote(
            summed.at[step, far_to],
            arrived.at[apart - 1, flip(far_index, step)],
            sum_send.at[step, apart - 1],
            sum_recv.at[step, apart - 1],
            place(far_to, near_index, tp_index),
        )

    def finish(step):
        total = part[step, :, tp_index].astype(jnp.float32)
        for other_tp in range(1, tp_count):
            part_copy(step, other_tp).wait_recv()
            total = total + other[step, other_tp - 1].astype(jnp.float32)
        summed[step] = total.astype(summed.dtype)
        for apart in range(1, far):
            sum_copy(step, apart).start()
        own_sum[flip(far_index, step)] = summed[step, far_index]

    for step in range(1, far):
        take((2,), step, 0)
        for role in relay_roles(step - 1):
            take((2,), step - 1, role)
    for role in relay_roles(far - 1):
        take((2,), far - 1, role)
    for step in range(far):
        take_group((2,), step)
        start = aligned(flip(far_index, step), chunk)
        product = lax.dot_general(
            hidden[...],
            down_all[pl.ds(start, chunk), :],
            (((1,), (1,)), ((), ())),
            preferred_element_type=jnp.float32,
        )
        part[step] = product.reshape(far, tp_count, own_rows, chunk).astype(part.dtype)
        for other_tp in range(1, tp_count):
            part_copy(step, other_tp).start()
        if step:
            finish(step - 1)
    finish(far - 1)

    for step in range(far):
        for apart in range(1, far):
            remote(
                summed.at[step, 0],
                arrived.at[apart - 1, flip(flip(far_index, apart), step)],
                sum_send.at[step, apart - 1],
                sum_recv.at[step, apart - 1],
                place(flip(far_index, apart), near_index, tp_index),
            ).wait_recv()
    for place_of in range(far):
        span = pl.ds(place_of * chunk, chunk)
        channel = own_sum[place_of].astype(jnp.float32)
        for apart in range(1, far):
            channel = channel + arrived[apart - 1, place_of].astype(jnp.float32)
        channel = channel.astype(jnp.bfloat16).astype(jnp.float32)
        out[:, span] = (stream[:, span].astype(jnp.float32) + 0.5 * channel).astype(out.dtype)

    for matrix in range(3):
        for step in range(1, far):
            by_count(
                tile_count(flip(far_index, step)),
                lambda number: far_copy(matrix, step, number).wait_send(),
            )
        for step in range(far):
            for role, bit in near_sends(step):
                by_count(
                    own_count,
                    lambda number: near_copy(matrix, step, role, bit, number).wait_send(),
                )
    for step in range(far):
        if step:
            rows_copy(step).wait_send()
        for other_tp in range(1, tp_count):
            pair_copy(step, other_tp).wait_send()
            part_copy(step, other_tp).wait_send()
        for apart in range(1, far):
            sum_copy(step, apart).wait_send()


def run_mixer(normed, stream, gate_weight, up_weight, down_weight, far, near, tp_count):
    own_rows, model = normed.shape
    depth, units = gate_weight.shape
    tiles = units // LANES
    wide = -(-tiles // far)
    width = wide * LANES
    chunk = near * depth
    row_total = far * tp_count * own_rows
    plan = (far, near, tp_count, depth, tiles, wide, width)
    bf16, f32 = jnp.bfloat16, jnp.float32
    others = max(tp_count - 1, 1)
    dma = pltpu.SemaphoreType.DMA
    vmem = pl.BlockSpec(memory_space=pltpu.VMEM)
    anywhere = pl.BlockSpec(memory_space=pl.ANY)
    return pl.pallas_call(
        functools.partial(mixer, plan),
        out_shape=jax.ShapeDtypeStruct((own_rows, model), bf16),
        in_specs=[vmem, vmem, anywhere, anywhere, anywhere],
        out_specs=vmem,
        scratch_shapes=[
            pltpu.VMEM((model, width), bf16),
            pltpu.VMEM((model, width), bf16),
            pltpu.VMEM((model, width), bf16),
            pltpu.VMEM((far, tp_count, own_rows, model), bf16),
            pltpu.VMEM((row_total, width), f32),
            pltpu.VMEM((row_total, width), f32),
            pltpu.VMEM((row_total, width), bf16),
            pltpu.VMEM((far, far, tp_count, own_rows, chunk), bf16),
            pltpu.VMEM((far, others, far, own_rows, chunk), bf16),
            pltpu.VMEM((far, far, own_rows, chunk), bf16),
            pltpu.VMEM((far - 1, far, own_rows, chunk), bf16),
            pltpu.VMEM((far, own_rows, chunk), bf16),
            dma((3,)),
            dma((3, far)),
            dma((3, far, near - 1)),
            dma((3, far, near)),
            dma((far,)),
            dma((far,)),
            dma((far, others)),
            dma((far, others)),
            dma((far, others)),
            dma((far, others)),
            dma((far, far - 1)),
            dma((far, far - 1)),
        ],
        compiler_params=pltpu.CompilerParams(
            collective_id=0, has_side_effects=True, vmem_limit_bytes=56 * 1024 * 1024
        ),
    )(normed, stream, gate_weight, up_weight, down_weight)


def shards(
    residual,
    query_small,
    query_large,
    latent,
    rope_key,
    key_up_small,
    value_up_small,
    key_up_large,
    value_up_large,
    out_small,
    out_large,
    norm_gain,
    gate_weight,
    up_weight,
    down_weight,
):
    row_count = query_small.shape[0]
    sp_count = lax.axis_size("sp")
    tp_count = lax.axis_size("tp")
    far = 1
    while far * far < sp_count:
        far *= 2
    near = sp_count // far
    sp_index = lax.axis_index("sp")
    tp_index = lax.axis_index("tp")

    def sp_swap(array, step):
        return lax.ppermute(array, "sp", [(i, i ^ step) for i in range(sp_count)])

    def bits_below(count):
        bits = []
        while 1 << len(bits) < count:
            bits.append(1 << len(bits))
        return bits

    def tp_swap(array, step):
        if step == 0:
            return array
        return lax.ppermute(array, "tp", [(i, i ^ step) for i in range(tp_count)])

    first_row = sp_index * row_count
    query_pos = first_row + jnp.arange(row_count, dtype=jnp.int32)
    heads_small = key_up_small.shape[1] // HEAD_SMALL
    heads_large = key_up_large.shape[1] // HEAD_LARGE
    latent_width = latent.shape[1]

    own_rows = row_count // tp_count
    own_keys = jnp.concatenate([latent, rotate(rope_key, query_pos)], axis=1)
    all_keys = lax.dynamic_slice_in_dim(own_keys, tp_index * own_rows, own_rows, 0)
    key_order = [0]
    for bit in reversed(bits_below(sp_count)):
        all_keys = jnp.concatenate([all_keys, sp_swap(all_keys, bit)], axis=0)
        key_order = key_order + [place ^ bit for place in key_order]
    all_keys = jnp.concatenate([tp_swap(all_keys, step) for step in range(tp_count)], axis=0)
    key_pos = jnp.concatenate(
        [
            (sp_index ^ place) * row_count
            + (tp_index ^ step) * own_rows
            + jnp.arange(own_rows, dtype=jnp.int32)
            for step in range(tp_count)
            for place in key_order
        ]
    )

    def split_query(query, head_count, head_size):
        shaped = query.reshape(row_count, head_count, head_size + ROPE)
        nope_part = jnp.transpose(shaped[..., :head_size], (1, 0, 2))
        turned = jnp.transpose(rotate(shaped[..., head_size:], query_pos), (1, 0, 2))
        return (nope_part, turned)

    nope_small, turned_small = split_query(query_small, heads_small, HEAD_SMALL)
    nope_large, turned_large = split_query(query_large, heads_large, HEAD_LARGE)

    part_latent = all_keys[:, :latent_width]
    turned_key = all_keys[:, latent_width:]
    visible = key_pos[None, :] <= query_pos[:, None]

    def lift(weight):
        return jnp.dot(part_latent, weight, preferred_element_type=jnp.float32).astype(
            jnp.bfloat16
        )

    attended_small = attend(
        nope_small, turned_small, lift(key_up_small), lift(value_up_small), turned_key, visible, HEAD_SMALL
    )
    attended_large = attend(
        nope_large, turned_large, lift(key_up_large), lift(value_up_large), turned_key, visible, HEAD_LARGE
    )
    share_mixed = jnp.dot(
        attended_small, out_small, preferred_element_type=jnp.float32
    ) + jnp.dot(attended_large, out_large, preferred_element_type=jnp.float32)
    share_mixed = share_mixed.reshape(tp_count, own_rows, share_mixed.shape[1])
    mixed = lax.dynamic_index_in_dim(share_mixed, tp_index, 0, False)
    for step in range(1, tp_count):
        sent = lax.dynamic_index_in_dim(share_mixed, tp_index ^ step, 0, False)
        mixed = mixed + tp_swap(sent.astype(jnp.bfloat16), step).astype(jnp.float32)
    mixed = mixed.astype(jnp.bfloat16)
    stream = (residual.astype(jnp.float32) + mixed.astype(jnp.float32)).astype(jnp.bfloat16)
    as_float = stream.astype(jnp.float32)
    normed = as_float * lax.rsqrt(jnp.mean(as_float * as_float, axis=-1, keepdims=True) + norm_eps)
    normed = (normed * norm_gain.astype(jnp.float32)[None, :]).astype(jnp.bfloat16)

    spare = -gate_weight.shape[1] % LANES
    if spare:
        gate_weight, up_weight, down_weight = (
            jnp.pad(weight, ((0, 0), (0, spare))) for weight in (gate_weight, up_weight, down_weight)
        )
    return run_mixer(normed, stream, gate_weight, up_weight, down_weight, far, near, tp_count)


def solution(mesh):
    placed = (
        P(("sp", "tp"), None),
        P("sp", "tp"),
        P("sp", "tp"),
        P("sp", None),
        P("sp", None),
        P(None, "tp"),
        P(None, "tp"),
        P(None, "tp"),
        P(None, "tp"),
        P("tp", None),
        P("tp", None),
        P(),
        P("sp", "tp"),
        P("sp", "tp"),
        P("sp", "tp"),
    )
    return jax.shard_map(
        shards, mesh=mesh, in_specs=placed, out_specs=P(("sp", "tp"), None), check_vma=False
    )
```

```python
import functools
import math

import jax
import jax.numpy as jnp
import numpy as np
from jax import lax
from jax.experimental import pallas as pl
from jax.experimental.pallas import tpu as pltpu
from jax.sharding import PartitionSpec as P

MESH = pl.DeviceIdType.MESH
HEAD_SMALL = 64
HEAD_LARGE = 128
ROPE = 32
LANES = 128


big_negative = -1e30
rope_base = 500000.0
norm_eps = 1e-06


def flip(index, mask):
    bit = 1
    while bit <= mask:
        if mask & bit:
            index = index + bit * (1 - 2 * lax.rem(lax.div(index, bit), 2))
        bit *= 2
    return index


def aligned(index, size):
    return pl.multiple_of(index * size, size)


def mixer(
    plan,
    residual,
    query_small,
    query_large,
    latent,
    rope_key,
    turn_rates,
    key_up_small,
    value_up_small,
    key_up_large,
    value_up_large,
    gain,
    out_small,
    out_large,
    gate,
    up,
    down,
    out,
    keys_all,
    queries,
    bias,
    attended_small,
    attended_large,
    out_small_held,
    out_large_held,
    mixed_part,
    mixed_other,
    stream,
    gate_all,
    up_all,
    down_all,
    rows_all,
    gate_sum,
    up_sum,
    hidden,
    part,
    other,
    summed,
    arrived,
    own_sum,
    copy_sem,
    out_sem,
    far_send,
    near_send,
    weight_recv,
    keys_send,
    keys_recv,
    mixed_send,
    mixed_recv,
    rows_send,
    rows_recv,
    pair_send,
    pair_recv,
    part_send,
    part_recv,
    sum_send,
    sum_recv,
):
    far, near, tp_count, depth, tiles, wide, width = plan
    own_rows, model = residual.shape
    row_count, latent_width = latent.shape
    near_bits = near.bit_length() - 1
    chunk = near * depth
    row_total = far * tp_count * own_rows
    sp_index = lax.axis_index("sp")
    tp_index = lax.axis_index("tp")
    far_index = lax.div(sp_index, near)
    near_index = lax.rem(sp_index, near)

    def place(far_to, near_to, tp_to):
        return {"sp": far_to * near + near_to, "tp": tp_to}

    def first_tile(far_to):
        return lax.div(far_to * tiles + lax.rem(tp_index, 2) * (far - 1), far)

    def tile_count(far_to):
        return first_tile(far_to + 1) - first_tile(far_to)

    def by_count(count, act):
        if tiles % far == 0:
            act(wide)
            return
        for number in (wide - 1, wide):
            if number:
                pl.when(count == number)(functools.partial(act, number))

    inputs = (gate, up, down)
    held = (gate_all, up_all, down_all)
    own_count = tile_count(far_index)

    def source(matrix, far_to, number):
        start = aligned(first_tile(far_to), LANES)
        return inputs[matrix].at[:, pl.ds(start, number * LANES)]

    def block(matrix, far_from, near_from, number):
        start = aligned(far_from * near + near_from, depth)
        return held[matrix].at[pl.ds(start, depth), pl.ds(0, number * LANES)]

    def remote(src, dst, send, recv, device):
        return pltpu.make_async_remote_copy(
            src_ref=src,
            dst_ref=dst,
            send_sem=send,
            recv_sem=recv,
            device_id=device,
            device_id_type=MESH,
        )

    def own_copy(matrix, number):
        return pltpu.make_async_copy(
            source(matrix, far_index, number),
            block(matrix, far_index, near_index, number),
            copy_sem.at[matrix],
        )

    def far_copy(matrix, step, number):
        far_to = flip(far_index, step)
        return remote(
            source(matrix, far_to, number),
            block(matrix, far_index, near_index, number),
            far_send.at[matrix, step],
            weight_recv.at[matrix, step, 0],
            place(far_to, near_index, tp_index),
        )

    def near_order(step):
        return [(step + number) % near_bits for number in range(near_bits)]

    def near_sends(step):
        order = near_order(step)
        sends = []
        for role in range(near):
            reached = max([order.index(b) for b in range(near_bits) if role >> b & 1], default=-1)
            for bit in order[reached + 1 :]:
                sends.append((role, bit))
        return sends

    def near_copy(matrix, step, role, bit, number):
        far_from = flip(far_index, step)
        near_from = flip(near_index, role)
        target = block(matrix, far_from, near_from, number)
        direct = step == 0 and role == 0
        return remote(
            source(matrix, far_index, number) if direct else target,
            target,
            near_send.at[matrix, step, near_sends(step).index((role, bit))],
            weight_recv.at[matrix, step, role | 1 << bit],
            place(far_index, flip(near_index, 1 << bit), tp_index),
        )

    def start_far(matrix, step):
        by_count(
            tile_count(flip(far_index, step)),
            lambda number: far_copy(matrix, step, number).start(),
        )

    def forward(matrix, step, role):
        def act(number):
            for sender, bit in near_sends(step):
                if sender == role:
                    near_copy(matrix, step, role, bit, number).start()

        by_count(own_count, act)

    def await_block(matrix, step, role):
        def act(number):
            if role == 0 and step == 0:
                own_copy(matrix, number).wait()
            else:
                far_from, near_from = flip(far_index, step), flip(near_index, role)
                target = block(matrix, far_from, near_from, number)
                remote(
                    target,
                    target,
                    copy_sem.at[matrix],
                    weight_recv.at[matrix, step, role],
                    place(far_index, flip(near_index, 1), tp_index),
                ).wait_recv()

        by_count(own_count, act)

    def relay_roles(step):
        return sorted({role for role, _ in near_sends(step) if role})

    done = set()

    def take(matrices, step, role):
        for matrix in matrices:
            if (matrix, step, role) not in done:
                done.add((matrix, step, role))
                await_block(matrix, step, role)
                if not (step == 0 and role == 0):
                    forward(matrix, step, role)

    def take_group(matrices, step):
        for role in range(near):
            take(matrices, step, role)

    rates = turn_rates[...]

    def turning(first, count):
        rows = first + lax.broadcasted_iota(jnp.int32, (count, 1), 0)
        angles = rows.astype(jnp.float32) * rates
        cosine, sine = jnp.cos(angles), jnp.sin(angles)
        return (
            jnp.concatenate([cosine, cosine], axis=1),
            jnp.concatenate([-sine, sine], axis=1),
        )

    def turned(vectors, table):
        half = vectors.shape[1] // 2
        vectors = vectors.astype(jnp.float32)
        swapped = jnp.concatenate([vectors[:, half:], vectors[:, :half]], axis=1)
        return vectors * table[0] + swapped * table[1]

    first_row = sp_index * row_count
    first_own = tp_index * own_rows
    held_rows = pl.ds(aligned(tp_index, own_rows), own_rows)
    key_turn = turned(rope_key[held_rows, :], turning(first_row + first_own, own_rows))
    key_turn = key_turn.astype(jnp.bfloat16)
    key_pad = jnp.zeros((own_rows, keys_all.shape[3] - latent_width - ROPE), jnp.bfloat16)
    keys_all[tp_index, sp_index] = jnp.concatenate(
        [latent[held_rows, :], key_turn, key_pad], axis=1
    )

    if tiles % far:
        spare = pl.ds((wide - 1) * LANES, LANES)

        @pl.when(own_count < wide)
        def _():
            gate_all[:, spare] = jnp.zeros((far * chunk, LANES), gate_all.dtype)
            up_all[:, spare] = jnp.zeros((far * chunk, LANES), up_all.dtype)
            down_all[:, spare] = jnp.zeros((far * chunk, LANES), down_all.dtype)

    barrier = pltpu.get_barrier_semaphore()
    peers = [place(flip(far_index, step), near_index, tp_index) for step in range(1, far)]
    peers += [place(far_index, flip(near_index, 1 << b), tp_index) for b in range(near_bits)]
    peers += [place(far_index, near_index, flip(tp_index, j)) for j in range(1, tp_count)]
    for peer in peers:
        pl.semaphore_signal(barrier, inc=1, device_id=peer, device_id_type=MESH)
    pl.semaphore_wait(barrier, len(peers))

    def key_block(step, role):
        return keys_all.at[tp_index, flip(far_index, step) * near + flip(near_index, role)]

    def key_far(step):
        return remote(
            key_block(0, 0),
            key_block(0, 0),
            keys_send.at[step, near - 1],
            keys_recv.at[step, 0],
            place(flip(far_index, step), near_index, tp_index),
        )

    def key_near(step, role, bit):
        return remote(
            key_block(step, role),
            key_block(step, role),
            keys_send.at[step, near_sends(step).index((role, bit))],
            keys_recv.at[step, role | 1 << bit],
            place(far_index, flip(near_index, 1 << bit), tp_index),
        )

    def key_forward(step, role):
        for sender, bit in near_sends(step):
            if sender == role:
                key_near(step, role, bit).start()

    def key_take(step, role):
        remote(
            key_block(step, role),
            key_block(step, role),
            copy_sem.at[0],
            keys_recv.at[step, role],
            place(far_index, flip(near_index, 1), tp_index),
        ).wait_recv()
        key_forward(step, role)

    def key_pair(step, other_tp):
        group = keys_all.at[tp_index, pl.ds(flip(far_index, step) * near, near)]
        return remote(
            group,
            group,
            mixed_send.at[step, other_tp - 1],
            mixed_recv.at[step, other_tp - 1],
            place(far_index, near_index, flip(tp_index, other_tp)),
        )

    pairs = (0, 1)
    for step in range(1, far):
        key_far(step).start()
    key_forward(0, 0)
    for step in range(1, far):
        for matrix in pairs:
            start_far(matrix, step)
    out_copies = [
        pltpu.make_async_copy(out_small, out_small_held, out_sem.at[0]),
        pltpu.make_async_copy(out_large, out_large_held, out_sem.at[1]),
    ]
    for copy in out_copies:
        copy.start()
    for matrix in range(3):
        by_count(own_count, lambda number: own_copy(matrix, number).start())

    groups = []
    query_table = turning(first_row, row_count)
    lifted = 0
    for query, key_up, value_up, attended, size in (
        (query_small, key_up_small, value_up_small, attended_small, HEAD_SMALL),
        (query_large, key_up_large, value_up_large, attended_large, HEAD_LARGE),
    ):
        span_width = size + ROPE
        heads = query.shape[1] // span_width
        scale = float(span_width) ** -0.5 * math.log2(math.e)
        pad = jnp.zeros((row_count, keys_all.shape[3] - latent_width - ROPE), jnp.bfloat16)
        for head in range(heads):
            vector = query[:, head * span_width : (head + 1) * span_width]
            content = lax.dot_general(
                vector[:, :size],
                key_up[:, head * size : (head + 1) * size],
                (((1,), (1,)), ((), ())),
                preferred_element_type=jnp.float32,
            )
            rotary = turned(vector[:, size:], query_table)
            queries[lifted * row_count : (lifted + 1) * row_count, :] = jnp.concatenate(
                [(content * scale).astype(jnp.bfloat16), (rotary * scale).astype(jnp.bfloat16), pad],
                axis=1,
            )
            if head % 2 == 0:
                groups.append((lifted, head, min(2, heads - head), size, value_up, attended))
            lifted += 1
    key_total = tp_count * far * near * own_rows
    number = lax.broadcasted_iota(jnp.int32, (1, key_total), 1)
    key_tp = lax.div(number, far * near * own_rows)
    key_rest = lax.rem(number, far * near * own_rows)
    key_pos = (
        lax.div(key_rest, own_rows) * row_count + key_tp * own_rows + lax.rem(key_rest, own_rows)
    )
    query_pos = first_row + lax.broadcasted_iota(jnp.int32, (row_count, 1), 0)
    bias[...] = jnp.where(key_pos <= query_pos, 0.0, big_negative)

    def key_group(step):
        for role in range(1, near):
            if role not in relay_roles(step):
                key_take(step, role)
        for other_tp in range(1, tp_count):
            key_pair(step, other_tp).start()

    for step in range(1, far):
        key_take(step, 0)
        for role in relay_roles(step - 1):
            key_take(step - 1, role)
        if step > 1:
            key_group(step - 2)
    for role in relay_roles(far - 1):
        key_take(far - 1, role)
    for matrix in pairs:
        forward(matrix, 0, 0)
    for step in range(max(far - 2, 0), far):
        key_group(step)
    for step in range(far):
        for other_tp in range(1, tp_count):
            key_pair(step, other_tp).wait_recv()

    relay_plan = []
    for step in range(1, far):
        relay_plan.append((step, 0))
        for role in relay_roles(step - 1):
            relay_plan.append((step - 1, role))
    for role in relay_roles(far - 1):
        relay_plan.append((far - 1, role))

    for index, (first_head, head, count, size, value_up, attended) in enumerate(groups):
        rows = pl.ds(first_head * row_count, count * row_count)
        keys = keys_all[...].reshape(key_total, keys_all.shape[3])
        scores = lax.dot_general(
            queries[rows, :], keys, (((1,), (1,)), ((), ())), preferred_element_type=jnp.float32
        )
        masked = scores.reshape(count, row_count, key_total) + bias[...][None]
        masked = masked.reshape(count * row_count, key_total)
        weights = jnp.exp2(masked - jnp.max(masked, axis=1, keepdims=True))
        totals = jnp.sum(weights, axis=1, keepdims=True)
        gathered = jnp.dot(
            weights.astype(jnp.bfloat16),
            keys[:, :latent_width],
            preferred_element_type=jnp.float32,
        )
        gathered = (gathered / totals).astype(jnp.bfloat16)
        values = [
            jnp.dot(
                gathered[place_of * row_count : (place_of + 1) * row_count],
                value_up[:, (head + place_of) * size : (head + place_of + 1) * size],
                preferred_element_type=jnp.float32,
            ).astype(jnp.bfloat16)
            for place_of in range(count)
        ]
        attended[:, head * size : (head + count) * size] = jnp.concatenate(values, axis=1)
        if relay_plan:
            take(pairs, *relay_plan.pop(0))

    for copy in out_copies:
        copy.wait()
    share = jnp.dot(
        attended_small[...], out_small_held[...], preferred_element_type=jnp.float32
    ) + jnp.dot(attended_large[...], out_large_held[...], preferred_element_type=jnp.float32)
    mixed_part[...] = share.reshape(tp_count, own_rows, model)

    def mixed_copy(other_tp):
        tp_to = flip(tp_index, other_tp)
        return remote(
            mixed_other.at[0, other_tp - 1],
            mixed_other.at[1, other_tp - 1],
            mixed_send.at[far, other_tp - 1],
            mixed_recv.at[far, other_tp - 1],
            place(far_index, near_index, tp_to),
        )

    for other_tp in range(1, tp_count):
        mixed_other[0, other_tp - 1] = mixed_part[flip(tp_index, other_tp)].astype(jnp.bfloat16)
        mixed_copy(other_tp).start()
    mixed = mixed_part[tp_index]
    for other_tp in range(1, tp_count):
        mixed_copy(other_tp).wait_recv()
        mixed = mixed + mixed_other[1, other_tp - 1].astype(jnp.float32)
    mixed = mixed.astype(jnp.bfloat16).astype(jnp.float32)
    stream[...] = (residual[...].astype(jnp.float32) + mixed).astype(jnp.bfloat16)
    as_float = stream[...].astype(jnp.float32)
    spread = lax.rsqrt(jnp.mean(as_float * as_float, axis=1, keepdims=True) + norm_eps)
    normed = as_float * spread * gain[...].astype(jnp.float32)
    rows_all[far_index, tp_index] = normed.astype(jnp.bfloat16)

    def rows_copy(step):
        return remote(
            rows_all.at[far_index, tp_index],
            rows_all.at[far_index, tp_index],
            rows_send.at[step],
            rows_recv.at[step],
            place(flip(far_index, step), near_index, tp_index),
        )

    def pair_copy(step, other_tp):
        far_from = flip(far_index, step)
        target = rows_all.at[far_from, tp_index]
        return remote(
            target,
            target,
            pair_send.at[step, other_tp - 1],
            pair_recv.at[step, other_tp - 1],
            place(far_index, near_index, flip(tp_index, other_tp)),
        )

    for step in range(1, far):
        rows_copy(step).start()
    for other_tp in range(1, tp_count):
        pair_copy(0, other_tp).start()

    for step in range(1, far):
        start_far(2, step)

    while relay_plan:
        take(pairs, *relay_plan.pop(0))
    forward(2, 0, 0)
    for step in range(1, far):
        rows_copy(step).wait_recv()
        for other_tp in range(1, tp_count):
            pair_copy(step, other_tp).start()
    for step in range(far):
        for other_tp in range(1, tp_count):
            pair_copy(step, other_tp).wait_recv()

    tile = 2 * LANES if width % (2 * LANES) == 0 else LANES
    for step in range(far):
        take_group(pairs, step)
        if step == far - 1:
            take((2,), 1, 0)
        start = aligned(flip(far_index, step), chunk)
        rows = rows_all[:, :, :, pl.ds(start, chunk)].reshape(row_total, chunk)
        for first in range(0, width, tile):
            span = pl.ds(first, tile)
            for weight, total in ((gate_all, gate_sum), (up_all, up_sum)):
                product = jnp.dot(
                    rows, weight[pl.ds(start, chunk), span], preferred_element_type=jnp.float32
                )
                total[:, span] = product if step == 0 else total[:, span] + product
    for first in range(0, width, LANES):
        span = pl.ds(first, LANES)
        value = gate_sum[:, span]
        value = (value / (1.0 + jnp.exp(-value)) * up_sum[:, span]).astype(hidden.dtype)
        if first >= (wide - 1) * LANES and tiles % far:
            value = jnp.where(own_count == wide, value, jnp.zeros_like(value))
        hidden[:, span] = value

    def part_copy(step, other_tp):
        tp_to = flip(tp_index, other_tp)
        return remote(
            part.at[step, :, tp_to],
            other.at[step, other_tp - 1],
            part_send.at[step, other_tp - 1],
            part_recv.at[step, other_tp - 1],
            place(far_index, near_index, tp_to),
        )

    def sum_copy(step, apart):
        far_to = flip(far_index, apart)
        return remote(
            summed.at[step, far_to],
            arrived.at[apart - 1, flip(far_index, step)],
            sum_send.at[step, apart - 1],
            sum_recv.at[step, apart - 1],
            place(far_to, near_index, tp_index),
        )

    def finish(step):
        total = part[step, :, tp_index].astype(jnp.float32)
        for other_tp in range(1, tp_count):
            part_copy(step, other_tp).wait_recv()
            total = total + other[step, other_tp - 1].astype(jnp.float32)
        summed[step] = total.astype(summed.dtype)
        for apart in range(1, far):
            sum_copy(step, apart).start()
        own_sum[flip(far_index, step)] = summed[step, far_index]

    for step in range(1, far):
        take((2,), step, 0)
        for role in relay_roles(step - 1):
            take((2,), step - 1, role)
    for role in relay_roles(far - 1):
        take((2,), far - 1, role)
    for step in range(far):
        take_group((2,), step)
        start = aligned(flip(far_index, step), chunk)
        product = lax.dot_general(
            hidden[...],
            down_all[pl.ds(start, chunk), :],
            (((1,), (1,)), ((), ())),
            preferred_element_type=jnp.float32,
        )
        part[step] = product.reshape(far, tp_count, own_rows, chunk).astype(part.dtype)
        for other_tp in range(1, tp_count):
            part_copy(step, other_tp).start()
        if step:
            finish(step - 1)
    finish(far - 1)

    for step in range(far):
        for apart in range(1, far):
            remote(
                summed.at[step, 0],
                arrived.at[apart - 1, flip(flip(far_index, apart), step)],
                sum_send.at[step, apart - 1],
                sum_recv.at[step, apart - 1],
                place(flip(far_index, apart), near_index, tp_index),
            ).wait_recv()
    for place_of in range(far):
        span = pl.ds(place_of * chunk, chunk)
        channel = own_sum[place_of].astype(jnp.float32)
        for apart in range(1, far):
            channel = channel + arrived[apart - 1, place_of].astype(jnp.float32)
        channel = channel.astype(jnp.bfloat16).astype(jnp.float32)
        out[:, span] = (stream[:, span].astype(jnp.float32) + 0.5 * channel).astype(out.dtype)

    for step in range(far):
        if step:
            key_far(step).wait_send()
        for role, bit in near_sends(step):
            key_near(step, role, bit).wait_send()
        for other_tp in range(1, tp_count):
            key_pair(step, other_tp).wait_send()
    for other_tp in range(1, tp_count):
        mixed_copy(other_tp).wait_send()
    for matrix in range(3):
        for step in range(1, far):
            by_count(
                tile_count(flip(far_index, step)),
                lambda number: far_copy(matrix, step, number).wait_send(),
            )
        for step in range(far):
            for role, bit in near_sends(step):
                by_count(
                    own_count,
                    lambda number: near_copy(matrix, step, role, bit, number).wait_send(),
                )
    for step in range(far):
        if step:
            rows_copy(step).wait_send()
        for other_tp in range(1, tp_count):
            pair_copy(step, other_tp).wait_send()
            part_copy(step, other_tp).wait_send()
        for apart in range(1, far):
            sum_copy(step, apart).wait_send()


def shards(
    residual,
    query_small,
    query_large,
    latent,
    rope_key,
    key_up_small,
    value_up_small,
    key_up_large,
    value_up_large,
    out_small,
    out_large,
    norm_gain,
    gate_weight,
    up_weight,
    down_weight,
):
    sp_count = lax.axis_size("sp")
    tp_count = lax.axis_size("tp")
    far = 1
    while far * far < sp_count:
        far *= 2
    near = sp_count // far
    spare = -gate_weight.shape[1] % LANES
    if spare:
        gate_weight, up_weight, down_weight = (
            jnp.pad(weight, ((0, 0), (0, spare))) for weight in (gate_weight, up_weight, down_weight)
        )
    own_rows, model = residual.shape
    row_count, latent_width = latent.shape
    depth, units = gate_weight.shape
    tiles = units // LANES
    wide = -(-tiles // far)
    width = wide * LANES
    chunk = near * depth
    row_total = far * tp_count * own_rows
    key_total = sp_count * row_count
    key_width = -(-(latent_width + ROPE) // LANES) * LANES
    small, large = out_small.shape[0], out_large.shape[0]
    heads = small // HEAD_SMALL + large // HEAD_LARGE
    rates = 1.0 / rope_base ** (np.arange(0, ROPE, 2, dtype=np.float32) / ROPE)
    plan = (far, near, tp_count, depth, tiles, wide, width)
    bf16, f32 = jnp.bfloat16, jnp.float32
    others = max(tp_count - 1, 1)
    dma = pltpu.SemaphoreType.DMA
    vmem = pl.BlockSpec(memory_space=pltpu.VMEM)
    anywhere = pl.BlockSpec(memory_space=pl.ANY)
    return pl.pallas_call(
        functools.partial(mixer, plan),
        out_shape=jax.ShapeDtypeStruct((own_rows, model), bf16),
        in_specs=[vmem] * 11 + [anywhere] * 5,
        out_specs=vmem,
        scratch_shapes=[
            pltpu.VMEM((tp_count, sp_count, own_rows, key_width), bf16),
            pltpu.VMEM((heads * row_count, key_width), bf16),
            pltpu.VMEM((row_count, key_total), f32),
            pltpu.VMEM((row_count, small), bf16),
            pltpu.VMEM((row_count, large), bf16),
            pltpu.VMEM(out_small.shape, bf16),
            pltpu.VMEM(out_large.shape, bf16),
            pltpu.VMEM((tp_count, own_rows, model), f32),
            pltpu.VMEM((2, others, own_rows, model), bf16),
            pltpu.VMEM((own_rows, model), bf16),
            pltpu.VMEM((model, width), bf16),
            pltpu.VMEM((model, width), bf16),
            pltpu.VMEM((model, width), bf16),
            pltpu.VMEM((far, tp_count, own_rows, model), bf16),
            pltpu.VMEM((row_total, width), f32),
            pltpu.VMEM((row_total, width), f32),
            pltpu.VMEM((row_total, width), bf16),
            pltpu.VMEM((far, far, tp_count, own_rows, chunk), bf16),
            pltpu.VMEM((far, others, far, own_rows, chunk), bf16),
            pltpu.VMEM((far, far, own_rows, chunk), bf16),
            pltpu.VMEM((far - 1, far, own_rows, chunk), bf16),
            pltpu.VMEM((far, own_rows, chunk), bf16),
            dma((3,)),
            dma((2,)),
            dma((3, far)),
            dma((3, far, near - 1)),
            dma((3, far, near)),
            dma((far, near)),
            dma((far, near)),
            dma((far + 1, others)),
            dma((far + 1, others)),
            dma((far,)),
            dma((far,)),
            dma((far, others)),
            dma((far, others)),
            dma((far, others)),
            dma((far, others)),
            dma((far, far - 1)),
            dma((far, far - 1)),
        ],
        compiler_params=pltpu.CompilerParams(
            collective_id=0, has_side_effects=True, vmem_limit_bytes=58 * 1024 * 1024
        ),
    )(
        residual,
        query_small,
        query_large,
        latent,
        rope_key,
        jnp.asarray(rates[None, :], f32),
        key_up_small,
        value_up_small,
        key_up_large,
        value_up_large,
        norm_gain[None, :],
        out_small,
        out_large,
        gate_weight,
        up_weight,
        down_weight,
    )


def solution(mesh):
    placed = (
        P(("sp", "tp"), None),
        P("sp", "tp"),
        P("sp", "tp"),
        P("sp", None),
        P("sp", None),
        P(None, "tp"),
        P(None, "tp"),
        P(None, "tp"),
        P(None, "tp"),
        P("tp", None),
        P("tp", None),
        P(),
        P("sp", "tp"),
        P("sp", "tp"),
        P("sp", "tp"),
    )
    return jax.shard_map(
        shards, mesh=mesh, in_specs=placed, out_specs=P(("sp", "tp"), None), check_vma=False
    )
```

```python
import functools
import math

import jax
import jax.numpy as jnp
import numpy as np
from jax import lax
from jax.experimental import pallas as pl
from jax.experimental.pallas import tpu as pltpu
from jax.sharding import PartitionSpec as P

MESH = pl.DeviceIdType.MESH
HEAD_SMALL = 64
HEAD_LARGE = 128
ROPE = 32
LANES = 128


big_negative = -1e30
rope_base = 500000.0
norm_eps = 1e-06


def flip(index, mask):
    bit = 1
    while bit <= mask:
        if mask & bit:
            index = index + bit * (1 - 2 * lax.rem(lax.div(index, bit), 2))
        bit *= 2
    return index


def aligned(index, size):
    return pl.multiple_of(index * size, size)


def mixer(
    plan,
    residual,
    query_small,
    query_large,
    latent,
    rope_key,
    turn_rates,
    key_up_small,
    value_up_small,
    key_up_large,
    value_up_large,
    gain,
    out_small,
    out_large,
    gate,
    up,
    down,
    out,
    keys_own,
    keys_all,
    queries,
    bias,
    attended_small,
    attended_large,
    out_small_held,
    out_large_held,
    mixed_part,
    mixed_other,
    stream,
    gate_all,
    up_all,
    down_all,
    rows_all,
    gate_sum,
    up_sum,
    hidden,
    part,
    other,
    summed,
    arrived,
    own_sum,
    copy_sem,
    out_sem,
    far_send,
    near_send,
    weight_recv,
    keys_send,
    keys_recv,
    mixed_send,
    mixed_recv,
    rows_send,
    rows_recv,
    pair_send,
    pair_recv,
    part_send,
    part_recv,
    sum_send,
    sum_recv,
):
    far, near, tp_count, depth, tiles, wide, width = plan
    own_rows, model = residual.shape
    row_count, latent_width = latent.shape
    near_bits = near.bit_length() - 1
    chunk = near * depth
    row_total = far * tp_count * own_rows
    sp_index = lax.axis_index("sp")
    tp_index = lax.axis_index("tp")
    far_index = lax.div(sp_index, near)
    near_index = lax.rem(sp_index, near)

    def place(far_to, near_to, tp_to):
        return {"sp": far_to * near + near_to, "tp": tp_to}

    def first_tile(far_to):
        return lax.div(far_to * tiles + lax.rem(tp_index, 2) * (far - 1), far)

    def tile_count(far_to):
        return first_tile(far_to + 1) - first_tile(far_to)

    def by_count(count, act):
        if tiles % far == 0:
            act(wide)
            return
        for number in (wide - 1, wide):
            if number:
                pl.when(count == number)(functools.partial(act, number))

    inputs = (gate, up, down)
    held = (gate_all, up_all, down_all)
    own_count = tile_count(far_index)

    def source(matrix, far_to, number):
        start = aligned(first_tile(far_to), LANES)
        return inputs[matrix].at[:, pl.ds(start, number * LANES)]

    def block(matrix, far_from, near_from, number):
        start = aligned(far_from * near + near_from, depth)
        return held[matrix].at[pl.ds(start, depth), pl.ds(0, number * LANES)]

    def remote(src, dst, send, recv, device):
        return pltpu.make_async_remote_copy(
            src_ref=src,
            dst_ref=dst,
            send_sem=send,
            recv_sem=recv,
            device_id=device,
            device_id_type=MESH,
        )

    def own_copy(matrix, number):
        return pltpu.make_async_copy(
            source(matrix, far_index, number),
            block(matrix, far_index, near_index, number),
            copy_sem.at[matrix],
        )

    def far_copy(matrix, step, number):
        far_to = flip(far_index, step)
        return remote(
            source(matrix, far_to, number),
            block(matrix, far_index, near_index, number),
            far_send.at[matrix, step],
            weight_recv.at[matrix, step, 0],
            place(far_to, near_index, tp_index),
        )

    def near_order(step):
        return [(step + number) % near_bits for number in range(near_bits)]

    def near_sends(step):
        order = near_order(step)
        sends = []
        for role in range(near):
            reached = max([order.index(b) for b in range(near_bits) if role >> b & 1], default=-1)
            for bit in order[reached + 1 :]:
                sends.append((role, bit))
        return sends

    def near_copy(matrix, step, role, bit, number):
        far_from = flip(far_index, step)
        near_from = flip(near_index, role)
        target = block(matrix, far_from, near_from, number)
        direct = step == 0 and role == 0
        return remote(
            source(matrix, far_index, number) if direct else target,
            target,
            near_send.at[matrix, step, near_sends(step + matrix).index((role, bit))],
            weight_recv.at[matrix, step, role | 1 << bit],
            place(far_index, flip(near_index, 1 << bit), tp_index),
        )

    def start_far(matrix, step):
        by_count(
            tile_count(flip(far_index, step)),
            lambda number: far_copy(matrix, step, number).start(),
        )

    def forward(matrix, step, role):
        def act(number):
            for sender, bit in near_sends(step + matrix):
                if sender == role:
                    near_copy(matrix, step, role, bit, number).start()

        by_count(own_count, act)

    def await_block(matrix, step, role):
        with jax.named_scope(f"wait_m{matrix}_s{step}_r{role}"):
            await_block_(matrix, step, role)

    def await_block_(matrix, step, role):
        def act(number):
            if role == 0 and step == 0:
                own_copy(matrix, number).wait()
            else:
                far_from, near_from = flip(far_index, step), flip(near_index, role)
                target = block(matrix, far_from, near_from, number)
                remote(
                    target,
                    target,
                    copy_sem.at[matrix],
                    weight_recv.at[matrix, step, role],
                    place(far_index, flip(near_index, 1), tp_index),
                ).wait_recv()

        by_count(own_count, act)

    def relay_roles(step):
        return sorted({role for role, _ in near_sends(step) if role})

    done = set()

    def take(matrices, step, role):
        for matrix in matrices:
            if (matrix, step, role) not in done:
                done.add((matrix, step, role))
                await_block(matrix, step, role)
                if not (step == 0 and role == 0):
                    forward(matrix, step, role)

    def relay(matrices, step):
        for matrix in matrices:
            for role in relay_roles(step + matrix):
                take((matrix,), step, role)

    def take_group(matrices, step):
        for role in range(near):
            take(matrices, step, role)

    barrier = pltpu.get_barrier_semaphore()
    peers = [place(flip(far_index, step), near_index, tp_index) for step in range(1, far)]
    peers += [place(far_index, flip(near_index, 1 << b), tp_index) for b in range(near_bits)]
    peers += [place(far_index, near_index, flip(tp_index, j)) for j in range(1, tp_count)]
    for peer in peers:
        pl.semaphore_signal(barrier, inc=1, device_id=peer, device_id_type=MESH)
    rates = turn_rates[...]

    def turning(first, count):
        rows = first + lax.broadcasted_iota(jnp.int32, (count, 1), 0)
        angles = rows.astype(jnp.float32) * rates
        cosine, sine = jnp.cos(angles), jnp.sin(angles)
        return (
            jnp.concatenate([cosine, cosine], axis=1),
            jnp.concatenate([-sine, sine], axis=1),
        )

    def turned(vectors, table):
        half = vectors.shape[1] // 2
        vectors = vectors.astype(jnp.float32)
        swapped = jnp.concatenate([vectors[:, half:], vectors[:, :half]], axis=1)
        return vectors * table[0] + swapped * table[1]

    first_row = sp_index * row_count
    query_table = turning(first_row, row_count)
    key_turn = turned(rope_key[...].T, query_table).astype(jnp.bfloat16)
    key_pad = jnp.zeros((row_count, keys_all.shape[3] - latent_width - ROPE), jnp.bfloat16)
    own_keys = jnp.concatenate([latent[...], key_turn, key_pad], axis=1)
    keys_own[...] = own_keys.reshape(tp_count, own_rows, keys_all.shape[3])
    keys_all[tp_index, sp_index] = keys_own[tp_index]

    if tiles % far:
        spare = pl.ds((wide - 1) * LANES, LANES)

        @pl.when(own_count < wide)
        def _():
            gate_all[:, spare] = jnp.zeros((far * chunk, LANES), gate_all.dtype)
            up_all[:, spare] = jnp.zeros((far * chunk, LANES), up_all.dtype)
            down_all[:, spare] = jnp.zeros((far * chunk, LANES), down_all.dtype)

    with jax.named_scope('barrier'):
        pl.semaphore_wait(barrier, len(peers))

    def key_block(step, role):
        return keys_all.at[tp_index, flip(far_index, step) * near + flip(near_index, role)]

    def key_far(step):
        return remote(
            key_block(0, 0),
            key_block(0, 0),
            keys_send.at[step, near - 1],
            keys_recv.at[step, 0],
            place(flip(far_index, step), near_index, tp_index),
        )

    def key_near(step, role, bit):
        return remote(
            key_block(step, role),
            key_block(step, role),
            keys_send.at[step, near_sends(step).index((role, bit))],
            keys_recv.at[step, role | 1 << bit],
            place(far_index, flip(near_index, 1 << bit), tp_index),
        )

    def key_forward(step, role):
        for sender, bit in near_sends(step):
            if sender == role:
                key_near(step, role, bit).start()

    def key_take(step, role):
      with jax.named_scope(f"wait_key_s{step}_r{role}"):
        remote(
            key_block(step, role),
            key_block(step, role),
            copy_sem.at[0],
            keys_recv.at[step, role],
            place(far_index, flip(near_index, 1), tp_index),
        ).wait_recv()
        key_forward(step, role)

    def key_pair(step, other_tp):
        group = keys_all.at[tp_index, pl.ds(flip(far_index, step) * near, near)]
        return remote(
            group,
            group,
            mixed_send.at[step, other_tp - 1],
            mixed_recv.at[step, other_tp - 1],
            place(far_index, near_index, flip(tp_index, other_tp)),
        )

    pairs = (0, 1)
    for step in range(1, far):
        key_far(step).start()
    key_forward(0, 0)
    for matrix in pairs:
        forward(matrix, 0, 0)
    for matrix in pairs:
        start_far(matrix, 1)
    inner = lax.rem(lax.div(far_index, max(far // 2, 1)) + lax.div(far_index, max(far // 4, 1)), 2)

    def start_rest(steps):
        for step in steps:
            for matrix in pairs:
                start_far(matrix, step)

    pl.when(inner == 0)(lambda: start_rest(range(2, far)))
    pl.when(inner == 1)(lambda: start_rest(range(far - 1, 1, -1)))
    start_far(2, 1)
    out_copies = [
        pltpu.make_async_copy(out_small, out_small_held, out_sem.at[0]),
        pltpu.make_async_copy(out_large, out_large_held, out_sem.at[1]),
    ]
    for copy in out_copies:
        copy.start()
    for matrix in range(3):
        by_count(own_count, lambda number: own_copy(matrix, number).start())

    groups = []
    lifted = 0
    for query, key_up, value_up, attended, size in (
        (query_small, key_up_small, value_up_small, attended_small, HEAD_SMALL),
        (query_large, key_up_large, value_up_large, attended_large, HEAD_LARGE),
    ):
        span_width = size + ROPE
        heads = query.shape[1] // span_width
        scale = float(span_width) ** -0.5 * math.log2(math.e)
        pad = jnp.zeros((row_count, keys_all.shape[3] - latent_width - ROPE), jnp.bfloat16)
        for head in range(heads):
            vector = query[:, head * span_width : (head + 1) * span_width]
            content = lax.dot_general(
                vector[:, :size],
                key_up[:, head * size : (head + 1) * size],
                (((1,), (1,)), ((), ())),
                preferred_element_type=jnp.float32,
            )
            rotary = turned(vector[:, size:], query_table)
            queries[lifted * row_count : (lifted + 1) * row_count, :] = jnp.concatenate(
                [(content * scale).astype(jnp.bfloat16), (rotary * scale).astype(jnp.bfloat16), pad],
                axis=1,
            )
            if head % 2 == 0:
                groups.append((lifted, head, min(2, heads - head), size, value_up, attended))
            lifted += 1
    key_total = tp_count * far * near * own_rows
    number = lax.broadcasted_iota(jnp.int32, (1, key_total), 1)
    key_tp = lax.div(number, far * near * own_rows)
    key_rest = lax.rem(number, far * near * own_rows)
    key_pos = (
        lax.div(key_rest, own_rows) * row_count + key_tp * own_rows + lax.rem(key_rest, own_rows)
    )
    query_pos = first_row + lax.broadcasted_iota(jnp.int32, (row_count, 1), 0)
    bias[...] = jnp.where(key_pos <= query_pos, 0.0, big_negative)

    def key_group(step):
        for role in range(1, near):
            if role not in relay_roles(step):
                key_take(step, role)
        for other_tp in range(1, tp_count):
            key_pair(step, other_tp).start()

    for step in range(1, far):
        key_take(step, 0)
        for role in relay_roles(step - 1):
            key_take(step - 1, role)
        if step > 1:
            key_group(step - 2)
    relay(pairs, 0)
    for role in relay_roles(far - 1):
        key_take(far - 1, role)
    take(pairs, 1, 0)
    forward(2, 0, 0)
    for step in range(max(far - 2, 0), far):
        key_group(step)
    for step in range(far):
        for other_tp in range(1, tp_count):
            with jax.named_scope('wait_keypair'):
                key_pair(step, other_tp).wait_recv()

    for index, (first_head, head, count, size, value_up, attended) in enumerate(groups):
        rows = pl.ds(first_head * row_count, count * row_count)
        keys = keys_all[...].reshape(key_total, keys_all.shape[3])
        scores = lax.dot_general(
            queries[rows, :], keys, (((1,), (1,)), ((), ())), preferred_element_type=jnp.float32
        )
        masked = scores.reshape(count, row_count, key_total) + bias[...][None]
        masked = masked.reshape(count * row_count, key_total)
        weights = jnp.exp2(masked - jnp.max(masked, axis=1, keepdims=True))
        totals = jnp.sum(weights, axis=1, keepdims=True)
        gathered = jnp.dot(
            weights.astype(jnp.bfloat16),
            keys[:, :latent_width],
            preferred_element_type=jnp.float32,
        )
        gathered = (gathered / totals).astype(jnp.bfloat16)
        values = [
            jnp.dot(
                gathered[place_of * row_count : (place_of + 1) * row_count],
                value_up[:, (head + place_of) * size : (head + place_of + 1) * size],
                preferred_element_type=jnp.float32,
            ).astype(jnp.bfloat16)
            for place_of in range(count)
        ]
        with jax.named_scope(f"att_done{index}"):
            attended[:, head * size : (head + count) * size] = jnp.concatenate(values, axis=1)
        if index == len(groups) - 1:
            relay(pairs, 1)

    for copy in out_copies:
        with jax.named_scope('outcopy'):
            copy.wait()
    share = jnp.dot(
        attended_small[...], out_small_held[...], preferred_element_type=jnp.float32
    ) + jnp.dot(attended_large[...], out_large_held[...], preferred_element_type=jnp.float32)
    mixed_part[...] = share.reshape(tp_count, own_rows, model)

    def mixed_copy(other_tp):
        tp_to = flip(tp_index, other_tp)
        return remote(
            mixed_other.at[0, other_tp - 1],
            mixed_other.at[1, other_tp - 1],
            mixed_send.at[far, other_tp - 1],
            mixed_recv.at[far, other_tp - 1],
            place(far_index, near_index, tp_to),
        )

    for other_tp in range(1, tp_count):
        mixed_other[0, other_tp - 1] = mixed_part[flip(tp_index, other_tp)].astype(jnp.bfloat16)
        mixed_copy(other_tp).start()
    for step in range(2, far):
        take(pairs, step, 0)
    mixed = mixed_part[tp_index]
    for other_tp in range(1, tp_count):
        with jax.named_scope('wait_mixed'):
            mixed_copy(other_tp).wait_recv()
        mixed = mixed + mixed_other[1, other_tp - 1].astype(jnp.float32)
    mixed = mixed.astype(jnp.bfloat16).astype(jnp.float32)
    stream[...] = (residual[...].astype(jnp.float32) + mixed).astype(jnp.bfloat16)
    as_float = stream[...].astype(jnp.float32)
    spread = lax.rsqrt(jnp.mean(as_float * as_float, axis=1, keepdims=True) + norm_eps)
    normed = as_float * spread * gain[...].astype(jnp.float32).reshape(1, model)
    with jax.named_scope('normed'):
        rows_all[far_index, tp_index] = normed.astype(jnp.bfloat16)

    far_bits = far.bit_length() - 1
    pieces = 2 if model % (2 * LANES) == 0 else 1
    piece_width = model // pieces

    def rows_sends():
        sends = []
        for role in range(far):
            low = min([b for b in range(far_bits) if role >> b & 1], default=far_bits)
            sends += [(role, bit) for bit in reversed(range(low))]
        return sends

    def rows_part(role, piece):
        span = pl.ds(piece * piece_width, piece_width)
        return rows_all.at[flip(far_index, role), tp_index, :, span]

    def rows_copy(role, bit, piece):
        return remote(
            rows_part(role, piece),
            rows_part(role, piece),
            rows_send.at[rows_sends().index((role, bit)), piece],
            rows_recv.at[role | 1 << bit, piece],
            place(flip(far_index, 1 << bit), near_index, tp_index),
        )

    def pair_copy(role, other_tp, piece):
        return remote(
            rows_part(role, piece),
            rows_part(role, piece),
            pair_send.at[role, other_tp - 1, piece],
            pair_recv.at[role, other_tp - 1, piece],
            place(far_index, near_index, flip(tp_index, other_tp)),
        )

    def rows_pass(role, piece):
        for sender, bit in rows_sends():
            if sender == role:
                rows_copy(role, bit, piece).start()
        for other_tp in range(1, tp_count):
            pair_copy(role, other_tp, piece).start()

    def rows_take(role):
        for piece in range(pieces):
            with jax.named_scope(f"wait_rows{role}_{piece}"):
                remote(
                    rows_part(role, piece),
                    rows_part(role, piece),
                    copy_sem.at[0],
                    rows_recv.at[role, piece],
                    place(flip(far_index, 1), near_index, tp_index),
                ).wait_recv()
            rows_pass(role, piece)

    for piece in range(pieces):
        rows_pass(0, piece)
    for step in reversed(range(3, far)):
        start_far(2, step)
    relayed = sorted({role for role, _ in rows_sends() if role}, reverse=True)
    leaves = [role for role in range(1, far) if role not in relayed]
    relay((2,), 0)
    for step in range(2, far // 2 + 1):
        relay(pairs, step)
    for role in relayed:
        rows_take(role)
    if far > 2:
        start_far(2, 2)
    for step in range(far // 2 + 1, far):
        relay(pairs, step)
    take((2,), 1, 0)
    for role in leaves:
        rows_take(role)
    for step in reversed(range(3, far)):
        take((2,), step, 0)
    for role in range(far):
        for other_tp in range(1, tp_count):
            for piece in range(pieces):
                with jax.named_scope(f"wait_pair{role}"):
                    pair_copy(role, other_tp, piece).wait_recv()

    tile = 2 * LANES if width % (2 * LANES) == 0 else LANES
    for step in range(far):
        take_group(pairs, step)
        start = aligned(flip(far_index, step), chunk)
        rows = rows_all[:, :, :, pl.ds(start, chunk)].reshape(row_total, chunk)
        for first in range(0, width, tile):
            span = pl.ds(first, tile)
            for weight, total in ((gate_all, gate_sum), (up_all, up_sum)):
                product = jnp.dot(
                    rows, weight[pl.ds(start, chunk), span], preferred_element_type=jnp.float32
                )
                total[:, span] = product if step == 0 else total[:, span] + product
    for first in range(0, width, LANES):
        span = pl.ds(first, LANES)
        value = gate_sum[:, span]
        value = (value / (1.0 + jnp.exp(-value)) * up_sum[:, span]).astype(hidden.dtype)
        if first >= (wide - 1) * LANES and tiles % far:
            value = jnp.where(own_count == wide, value, jnp.zeros_like(value))
        hidden[:, span] = value

    half = chunk // 2

    def columns_of(step, side):
        top = near // 2
        return flip(far_index, step) * 2 + lax.rem(lax.div(near_index, top) + side, 2)

    def part_copy(step, side, other_tp):
        tp_to = flip(tp_index, other_tp)
        return remote(
            part.at[step * 2 + side, :, tp_to],
            other.at[step * 2 + side, other_tp - 1],
            part_send.at[step * 2 + side, other_tp - 1],
            part_recv.at[step * 2 + side, other_tp - 1],
            place(far_index, near_index, tp_to),
        )

    def sum_copy(step, side, apart):
        far_to = flip(far_index, apart)
        return remote(
            summed.at[step * 2 + side, far_to],
            arrived.at[apart - 1, columns_of(step, side)],
            sum_send.at[step * 2 + side, apart - 1],
            sum_recv.at[step * 2 + side, apart - 1],
            place(far_to, near_index, tp_index),
        )

    def finish(step, side):
        total = part[step * 2 + side, :, tp_index].astype(jnp.float32)
        for other_tp in range(1, tp_count):
            with jax.named_scope(f"wait_part{step}_{side}"):
                part_copy(step, side, other_tp).wait_recv()
            total = total + other[step * 2 + side, other_tp - 1].astype(jnp.float32)
        summed[step * 2 + side] = total.astype(summed.dtype)
        for apart in range(1, far):
            sum_copy(step, side, apart).start()
        own_sum[columns_of(step, side)] = summed[step * 2 + side, far_index]

    def down_part(step, side):
        for role in range(side * near // 2, (side + 1) * near // 2):
            take((2,), step, role)
        start = aligned(columns_of(step, side), half)
        product = lax.dot_general(
            hidden[...],
            down_all[pl.ds(start, half), :],
            (((1,), (1,)), ((), ())),
            preferred_element_type=jnp.float32,
        )
        with jax.named_scope(f"downdot{step}_{side}"):
            part[step * 2 + side] = product.reshape(far, tp_count, own_rows, half).astype(part.dtype)
        for other_tp in range(1, tp_count):
            part_copy(step, side, other_tp).start()

    if far > 2:
        take((2,), 2, 0)
    relay((2,), 1)
    order = [0, 1] + list(reversed(range(2, far)))
    parts = [(step, side) for step in order for side in range(2)]
    for number, (step, side) in enumerate(parts):
        if side == 0:
            for later in order[order.index(step) + 1 :][:1]:
                take((2,), later, 0)
                relay((2,), later)
        down_part(step, side)
        if number:
            finish(*parts[number - 1])
    finish(*parts[-1])

    for step, side in parts:
        for apart in range(1, far):
            with jax.named_scope(f"wait_sum{step}_{side}_{apart}"):
                remote(
                    summed.at[step * 2 + side, 0],
                    arrived.at[apart - 1, columns_of(step, side)],
                    sum_send.at[step * 2 + side, apart - 1],
                    sum_recv.at[step * 2 + side, apart - 1],
                    place(flip(far_index, apart), near_index, tp_index),
                ).wait_recv()
    for place_of in range(2 * far):
        span = pl.ds(place_of * half, half)
        channel = own_sum[place_of].astype(jnp.float32)
        for apart in range(1, far):
            channel = channel + arrived[apart - 1, place_of].astype(jnp.float32)
        channel = channel.astype(jnp.bfloat16).astype(jnp.float32)
        out[:, span] = (stream[:, span].astype(jnp.float32) + 0.5 * channel).astype(out.dtype)

    for step in range(far):
        if step:
            key_far(step).wait_send()
        for role, bit in near_sends(step):
            key_near(step, role, bit).wait_send()
        for other_tp in range(1, tp_count):
            key_pair(step, other_tp).wait_send()
    for other_tp in range(1, tp_count):
        mixed_copy(other_tp).wait_send()
    for matrix in range(3):
        for step in range(1, far):
            by_count(
                tile_count(flip(far_index, step)),
                lambda number: far_copy(matrix, step, number).wait_send(),
            )
        for step in range(far):
            for role, bit in near_sends(step + matrix):
                by_count(
                    own_count,
                    lambda number: near_copy(matrix, step, role, bit, number).wait_send(),
                )
    for role, bit in rows_sends():
        for piece in range(pieces):
            rows_copy(role, bit, piece).wait_send()
    for step in range(far):
        for other_tp in range(1, tp_count):
            for piece in range(pieces):
                pair_copy(step, other_tp, piece).wait_send()
    for step, side in parts:
        for other_tp in range(1, tp_count):
            part_copy(step, side, other_tp).wait_send()
        for apart in range(1, far):
            sum_copy(step, side, apart).wait_send()


def shards(
    residual,
    query_small,
    query_large,
    latent,
    rope_key,
    key_up_small,
    value_up_small,
    key_up_large,
    value_up_large,
    out_small,
    out_large,
    norm_gain,
    gate_weight,
    up_weight,
    down_weight,
):
    sp_count = lax.axis_size("sp")
    tp_count = lax.axis_size("tp")
    far = 1
    while far * far < sp_count:
        far *= 2
    near = sp_count // far
    spare = -gate_weight.shape[1] % LANES
    if spare:
        gate_weight, up_weight, down_weight = (
            jnp.pad(weight, ((0, 0), (0, spare))) for weight in (gate_weight, up_weight, down_weight)
        )
    own_rows, model = residual.shape
    row_count, latent_width = latent.shape
    depth, units = gate_weight.shape
    tiles = units // LANES
    wide = -(-tiles // far)
    width = wide * LANES
    chunk = near * depth
    row_total = far * tp_count * own_rows
    key_total = sp_count * row_count
    key_width = -(-(latent_width + ROPE) // LANES) * LANES
    small, large = out_small.shape[0], out_large.shape[0]
    heads = small // HEAD_SMALL + large // HEAD_LARGE
    rates = 1.0 / rope_base ** (np.arange(0, ROPE, 2, dtype=np.float32) / ROPE)
    plan = (far, near, tp_count, depth, tiles, wide, width)
    bf16, f32 = jnp.bfloat16, jnp.float32
    others = max(tp_count - 1, 1)
    dma = pltpu.SemaphoreType.DMA
    vmem = pl.BlockSpec(memory_space=pltpu.VMEM)
    anywhere = pl.BlockSpec(memory_space=pl.ANY)
    return pl.pallas_call(
        functools.partial(mixer, plan),
        out_shape=jax.ShapeDtypeStruct((own_rows, model), bf16),
        in_specs=[vmem] * 11 + [anywhere] * 5,
        out_specs=vmem,
        scratch_shapes=[
            pltpu.VMEM((tp_count, own_rows, key_width), bf16),
            pltpu.VMEM((tp_count, sp_count, own_rows, key_width), bf16),
            pltpu.VMEM((heads * row_count, key_width), bf16),
            pltpu.VMEM((row_count, key_total), f32),
            pltpu.VMEM((row_count, small), bf16),
            pltpu.VMEM((row_count, large), bf16),
            pltpu.VMEM(out_small.shape, bf16),
            pltpu.VMEM(out_large.shape, bf16),
            pltpu.VMEM((tp_count, own_rows, model), f32),
            pltpu.VMEM((2, others, own_rows, model), bf16),
            pltpu.VMEM((own_rows, model), bf16),
            pltpu.VMEM((model, width), bf16),
            pltpu.VMEM((model, width), bf16),
            pltpu.VMEM((model, width), bf16),
            pltpu.VMEM((far, tp_count, own_rows, model), bf16),
            pltpu.VMEM((row_total, width), f32),
            pltpu.VMEM((row_total, width), f32),
            pltpu.VMEM((row_total, width), bf16),
            pltpu.VMEM((2 * far, far, tp_count, own_rows, chunk // 2), bf16),
            pltpu.VMEM((2 * far, others, far, own_rows, chunk // 2), bf16),
            pltpu.VMEM((2 * far, far, own_rows, chunk // 2), bf16),
            pltpu.VMEM((far - 1, 2 * far, own_rows, chunk // 2), bf16),
            pltpu.VMEM((2 * far, own_rows, chunk // 2), bf16),
            dma((3,)),
            dma((2,)),
            dma((3, far)),
            dma((3, far, near - 1)),
            dma((3, far, near)),
            dma((far, near)),
            dma((far, near)),
            dma((far + 1, others)),
            dma((far + 1, others)),
            dma((far - 1, 2)),
            dma((far, 2)),
            dma((far, others, 2)),
            dma((far, others, 2)),
            dma((2 * far, others)),
            dma((2 * far, others)),
            dma((2 * far, far - 1)),
            dma((2 * far, far - 1)),
        ],
        compiler_params=pltpu.CompilerParams(
            collective_id=0, has_side_effects=True, vmem_limit_bytes=58 * 1024 * 1024
        ),
    )(
        residual,
        query_small,
        query_large,
        latent,
        rope_key.T,
        jnp.asarray(rates[None, :], f32),
        key_up_small,
        value_up_small,
        key_up_large,
        value_up_large,
        norm_gain,
        out_small,
        out_large,
        gate_weight,
        up_weight,
        down_weight,
    )


def solution(mesh):
    placed = (
        P(("sp", "tp"), None),
        P("sp", "tp"),
        P("sp", "tp"),
        P("sp", None),
        P("sp", None),
        P(None, "tp"),
        P(None, "tp"),
        P(None, "tp"),
        P(None, "tp"),
        P("tp", None),
        P("tp", None),
        P(),
        P("sp", "tp"),
        P("sp", "tp"),
        P("sp", "tp"),
    )
    return jax.shard_map(
        shards, mesh=mesh, in_specs=placed, out_specs=P(("sp", "tp"), None), check_vma=False
    )
```

```python
import functools
import math

import jax
import jax.numpy as jnp
import numpy as np
from jax import lax
from jax.experimental import pallas as pl
from jax.experimental.pallas import tpu as pltpu
from jax.sharding import PartitionSpec as P

MESH = pl.DeviceIdType.MESH
HEAD_SMALL = 64
HEAD_LARGE = 128
ROPE = 32
LANES = 128


big_negative = -1e30
rope_base = 500000.0
norm_eps = 1e-06


def flip(index, mask):
    bit = 1
    while bit <= mask:
        if mask & bit:
            index = index + bit * (1 - 2 * lax.rem(lax.div(index, bit), 2))
        bit *= 2
    return index


def aligned(index, size):
    return pl.multiple_of(index * size, size)


def mixer(
    plan,
    residual_in,
    query_small_in,
    query_large_in,
    latent_in,
    rope_key_in,
    turn_rates_in,
    key_up_small_in,
    value_up_small_in,
    key_up_large_in,
    value_up_large_in,
    gain_in,
    out_small,
    out_large,
    gate,
    up,
    down,
    out,
    residual,
    query_small,
    query_large,
    latent,
    rope_key,
    turn_rates,
    key_up_small,
    value_up_small,
    key_up_large,
    value_up_large,
    gain,
    keys_own,
    keys_all,
    queries,
    bias,
    attended_small,
    attended_large,
    out_small_held,
    out_large_held,
    mixed_part,
    mixed_other,
    stream,
    gate_all,
    up_all,
    down_all,
    rows_all,
    gate_sum,
    up_sum,
    hidden,
    part,
    other,
    summed,
    arrived,
    own_sum,
    copy_sem,
    out_sem,
    small_sem,
    far_send,
    near_send,
    weight_recv,
    keys_send,
    keys_recv,
    mixed_send,
    mixed_recv,
    rows_send,
    rows_recv,
    pair_send,
    pair_recv,
    part_send,
    part_recv,
    sum_send,
    sum_recv,
):
    far, near, tp_count, depth, tiles, wide, width = plan
    own_rows, model = residual.shape
    row_count, latent_width = latent.shape
    near_bits = near.bit_length() - 1
    chunk = near * depth
    row_total = far * tp_count * own_rows
    sp_index = lax.axis_index("sp")
    tp_index = lax.axis_index("tp")
    far_index = lax.div(sp_index, near)
    near_index = lax.rem(sp_index, near)

    def place(far_to, near_to, tp_to):
        return {"sp": far_to * near + near_to, "tp": tp_to}

    def first_tile(far_to):
        return lax.div(far_to * tiles + lax.rem(tp_index, 2) * (far - 1), far)

    def tile_count(far_to):
        return first_tile(far_to + 1) - first_tile(far_to)

    def by_count(count, act):
        if tiles % far == 0:
            act(wide)
            return
        for number in (wide - 1, wide):
            if number:
                pl.when(count == number)(functools.partial(act, number))

    inputs = (gate, up, down)
    held = (gate_all, up_all, down_all)
    own_count = tile_count(far_index)

    def source(matrix, far_to, number):
        start = aligned(first_tile(far_to), LANES)
        return inputs[matrix].at[:, pl.ds(start, number * LANES)]

    def block(matrix, far_from, near_from, number):
        start = aligned(far_from * near + near_from, depth)
        return held[matrix].at[pl.ds(start, depth), pl.ds(0, number * LANES)]

    def remote(src, dst, send, recv, device):
        return pltpu.make_async_remote_copy(
            src_ref=src,
            dst_ref=dst,
            send_sem=send,
            recv_sem=recv,
            device_id=device,
            device_id_type=MESH,
        )

    def own_copy(matrix, number):
        return pltpu.make_async_copy(
            source(matrix, far_index, number),
            block(matrix, far_index, near_index, number),
            copy_sem.at[matrix],
        )

    def far_copy(matrix, step, number):
        far_to = flip(far_index, step)
        return remote(
            source(matrix, far_to, number),
            block(matrix, far_index, near_index, number),
            far_send.at[matrix],
            weight_recv.at[slot(matrix, step, 0)],
            place(far_to, near_index, tp_index),
        )

    def near_order(step):
        return [(step + number) % near_bits for number in range(near_bits)]

    def near_sends(step):
        order = near_order(step)
        sends = []
        for role in range(near):
            reached = max([order.index(b) for b in range(near_bits) if role >> b & 1], default=-1)
            for bit in order[reached + 1 :]:
                sends.append((role, bit))
        return sends

    slots = {}

    def is_leaf(matrix, step, role):
        return role > 0 and all(sender != role for sender, _ in near_sends(step + matrix))

    def slot(matrix, step, role):
        shared = matrix < 2 and is_leaf(matrix, step, role)
        return slots.setdefault(("leaf", step) if shared else (matrix, step, role), len(slots))

    def near_copy(matrix, step, role, bit, number):
        far_from = flip(far_index, step)
        near_from = flip(near_index, role)
        target = block(matrix, far_from, near_from, number)
        direct = step == 0 and role == 0
        return remote(
            source(matrix, far_index, number) if direct else target,
            target,
            near_send.at[matrix],
            weight_recv.at[slot(matrix, step, role | 1 << bit)],
            place(far_index, flip(near_index, 1 << bit), tp_index),
        )

    def start_far(matrix, step):
        by_count(
            tile_count(flip(far_index, step)),
            lambda number: far_copy(matrix, step, number).start(),
        )

    def forward(matrix, step, role):
        def act(number):
            for sender, bit in near_sends(step + matrix):
                if sender == role:
                    near_copy(matrix, step, role, bit, number).start()

        by_count(own_count, act)

    def await_block(matrix, step, role):
        with jax.named_scope(f"wait_m{matrix}_s{step}_r{role}"):
            await_block_(matrix, step, role)

    def await_block_(matrix, step, role):
        def act(number):
            if role == 0 and step == 0:
                own_copy(matrix, number).wait()
            else:
                far_from, near_from = flip(far_index, step), flip(near_index, role)
                target = block(matrix, far_from, near_from, number)
                remote(
                    target,
                    target,
                    copy_sem.at[matrix],
                    weight_recv.at[slot(matrix, step, role)],
                    place(far_index, flip(near_index, 1), tp_index),
                ).wait_recv()

        by_count(own_count, act)

    def relay_roles(step):
        return sorted({role for role, _ in near_sends(step) if role})

    done = set()

    def take(matrices, step, role):
        for matrix in matrices:
            if (matrix, step, role) not in done:
                done.add((matrix, step, role))
                await_block(matrix, step, role)
                if not (step == 0 and role == 0):
                    forward(matrix, step, role)

    def relay(matrices, step):
        for matrix in matrices:
            for role in relay_roles(step + matrix):
                take((matrix,), step, role)

    def take_group(matrices, step):
        leaves_of = [
            (matrix, role)
            for matrix in matrices
            for role in range(near)
            if is_leaf(matrix, step, role)
        ]
        for matrix in matrices:
            for role in range(near):
                if (matrix, role) not in leaves_of:
                    take((matrix,), step, role)

        def act(number):
            rows = gate_all.at[pl.ds(0, len(leaves_of) * depth), pl.ds(0, number * LANES)]
            pltpu.make_async_copy(rows, rows, weight_recv.at[slot(*shared)]).wait()

        shared = (leaves_of[0][0], step, leaves_of[0][1])
        with jax.named_scope(f"wait_leaves_s{step}"):
            by_count(own_count, act)

    barrier = pltpu.get_barrier_semaphore()
    peers = [place(flip(far_index, step), near_index, tp_index) for step in range(1, far)]
    peers += [place(far_index, flip(near_index, 1 << b), tp_index) for b in range(near_bits)]
    peers += [place(far_index, near_index, flip(tp_index, j)) for j in range(1, tp_count)]
    for peer in peers:
        pl.semaphore_signal(barrier, inc=1, device_id=peer, device_id_type=MESH)
    loads = [
        pltpu.make_async_copy(source_ref, held_ref, small_sem.at[place_of])
        for place_of, (source_ref, held_ref) in enumerate(
            (
                (residual_in, residual),
                (query_small_in, query_small),
                (query_large_in, query_large),
                (latent_in, latent),
                (rope_key_in, rope_key),
                (turn_rates_in, turn_rates),
                (key_up_small_in, key_up_small),
                (value_up_small_in, value_up_small),
                (key_up_large_in, key_up_large),
                (value_up_large_in, value_up_large),
                (gain_in, gain),
            )
        )
    ]
    first_loads = (3, 4, 5)
    for number in first_loads:
        loads[number].start()
    for number, load in enumerate(loads):
        if number not in first_loads:
            load.start()
    for number in first_loads:
        loads[number].wait()

    rates = turn_rates[...]

    def turning(first, count):
        rows = first + lax.broadcasted_iota(jnp.int32, (count, 1), 0)
        angles = rows.astype(jnp.float32) * rates
        cosine, sine = jnp.cos(angles), jnp.sin(angles)
        return (
            jnp.concatenate([cosine, cosine], axis=1),
            jnp.concatenate([-sine, sine], axis=1),
        )

    def turned(vectors, table):
        half = vectors.shape[1] // 2
        vectors = vectors.astype(jnp.float32)
        swapped = jnp.concatenate([vectors[:, half:], vectors[:, :half]], axis=1)
        return vectors * table[0] + swapped * table[1]

    first_row = sp_index * row_count
    query_table = turning(first_row, row_count)
    key_turn = turned(rope_key[...].T, query_table).astype(jnp.bfloat16)
    key_pad = jnp.zeros((row_count, keys_all.shape[3] - latent_width - ROPE), jnp.bfloat16)
    own_keys = jnp.concatenate([latent[...], key_turn, key_pad], axis=1)
    keys_own[...] = own_keys.reshape(tp_count, own_rows, keys_all.shape[3])
    keys_all[tp_index, sp_index] = keys_own[tp_index]

    if tiles % far:
        spare = pl.ds((wide - 1) * LANES, LANES)

        @pl.when(own_count < wide)
        def _():
            gate_all[:, spare] = jnp.zeros((far * chunk, LANES), gate_all.dtype)
            up_all[:, spare] = jnp.zeros((far * chunk, LANES), up_all.dtype)
            down_all[:, spare] = jnp.zeros((far * chunk, LANES), down_all.dtype)

    with jax.named_scope('barrier'):
        pl.semaphore_wait(barrier, len(peers))

    def key_block(step, role):
        return keys_all.at[tp_index, flip(far_index, step) * near + flip(near_index, role)]

    def key_far(step):
        return remote(
            key_block(0, 0),
            key_block(0, 0),
            keys_send.at[0],
            keys_recv.at[step, 0],
            place(flip(far_index, step), near_index, tp_index),
        )

    def key_slot(step, role):
        if role == 0:
            return step, 0
        return (step, 1 + relay_roles(step).index(role)) if role in relay_roles(step) else (0, 0)

    def key_near(step, role, bit):
        return remote(
            key_block(step, role),
            key_block(step, role),
            keys_send.at[0],
            keys_recv.at[key_slot(step, role | 1 << bit)],
            place(far_index, flip(near_index, 1 << bit), tp_index),
        )

    def key_forward(step, role):
        for sender, bit in near_sends(step):
            if sender == role:
                key_near(step, role, bit).start()

    def key_take(step, role):
      with jax.named_scope(f"wait_key_s{step}_r{role}"):
        remote(
            key_block(step, role),
            key_block(step, role),
            copy_sem.at[0],
            keys_recv.at[key_slot(step, role)],
            place(far_index, flip(near_index, 1), tp_index),
        ).wait_recv()
        key_forward(step, role)

    def key_pair(other_tp):
        return remote(
            keys_all.at[tp_index],
            keys_all.at[tp_index],
            mixed_send.at[0, other_tp - 1],
            mixed_recv.at[0, other_tp - 1],
            place(far_index, near_index, flip(tp_index, other_tp)),
        )

    pairs = (0, 1)
    for step in range(1, far):
        key_far(step).start()
    key_forward(0, 0)
    for matrix in pairs:
        forward(matrix, 0, 0)
    for matrix in pairs:
        start_far(matrix, 1)
    inner = lax.rem(lax.div(far_index, max(far // 2, 1)) + lax.div(far_index, max(far // 4, 1)), 2)

    def start_rest(steps):
        for step in steps:
            for matrix in pairs:
                start_far(matrix, step)

    pl.when(inner == 0)(lambda: start_rest(range(2, far)))
    pl.when(inner == 1)(lambda: start_rest(range(far - 1, 1, -1)))
    start_far(2, 1)
    out_copies = [
        pltpu.make_async_copy(out_small, out_small_held, out_sem.at[0]),
        pltpu.make_async_copy(out_large, out_large_held, out_sem.at[1]),
    ]
    for copy in out_copies:
        copy.start()
    for matrix in range(3):
        by_count(own_count, lambda number: own_copy(matrix, number).start())

    for number, load in enumerate(loads):
        if number not in first_loads:
            load.wait()

    groups = []
    lifted = 0
    for query, key_up, value_up, attended, size in (
        (query_small, key_up_small, value_up_small, attended_small, HEAD_SMALL),
        (query_large, key_up_large, value_up_large, attended_large, HEAD_LARGE),
    ):
        span_width = size + ROPE
        heads = query.shape[1] // span_width
        scale = float(span_width) ** -0.5 * math.log2(math.e)
        pad = jnp.zeros((row_count, keys_all.shape[3] - latent_width - ROPE), jnp.bfloat16)
        for head in range(heads):
            vector = query[:, head * span_width : (head + 1) * span_width]
            content = lax.dot_general(
                vector[:, :size],
                key_up[:, head * size : (head + 1) * size],
                (((1,), (1,)), ((), ())),
                preferred_element_type=jnp.float32,
            )
            rotary = turned(vector[:, size:], query_table)
            queries[lifted * row_count : (lifted + 1) * row_count, :] = jnp.concatenate(
                [(content * scale).astype(jnp.bfloat16), (rotary * scale).astype(jnp.bfloat16), pad],
                axis=1,
            )
            if head % 2 == 0:
                groups.append((lifted, head, min(2, heads - head), size, value_up, attended))
            lifted += 1
    key_total = tp_count * far * near * own_rows
    number = lax.broadcasted_iota(jnp.int32, (1, key_total), 1)
    key_tp = lax.div(number, far * near * own_rows)
    key_rest = lax.rem(number, far * near * own_rows)
    key_pos = (
        lax.div(key_rest, own_rows) * row_count + key_tp * own_rows + lax.rem(key_rest, own_rows)
    )
    query_pos = first_row + lax.broadcasted_iota(jnp.int32, (row_count, 1), 0)
    bias[...] = jnp.where(key_pos <= query_pos, 0.0, big_negative)

    for step in range(1, far):
        key_take(step, 0)
        for role in relay_roles(step - 1):
            key_take(step - 1, role)
    relay(pairs, 0)
    for role in relay_roles(far - 1):
        key_take(far - 1, role)
    take(pairs, 1, 0)
    forward(2, 0, 0)
    key_leaves = far * near - far - sum(len(relay_roles(step)) for step in range(far))
    leaf_blocks = keys_all.at[0, pl.ds(0, key_leaves)]
    with jax.named_scope("wait_keyleaves"):
        pltpu.make_async_copy(leaf_blocks, leaf_blocks, keys_recv.at[0, 0]).wait()
    for other_tp in range(1, tp_count):
        key_pair(other_tp).start()
    for other_tp in range(1, tp_count):
        with jax.named_scope("wait_keypair"):
            key_pair(other_tp).wait_recv()

    for index, (first_head, head, count, size, value_up, attended) in enumerate(groups):
        rows = pl.ds(first_head * row_count, count * row_count)
        keys = keys_all[...].reshape(key_total, keys_all.shape[3])
        scores = lax.dot_general(
            queries[rows, :], keys, (((1,), (1,)), ((), ())), preferred_element_type=jnp.float32
        )
        masked = scores.reshape(count, row_count, key_total) + bias[...][None]
        masked = masked.reshape(count * row_count, key_total)
        weights = jnp.exp2(masked - jnp.max(masked, axis=1, keepdims=True))
        totals = jnp.sum(weights, axis=1, keepdims=True)
        gathered = jnp.dot(
            weights.astype(jnp.bfloat16),
            keys[:, :latent_width],
            preferred_element_type=jnp.float32,
        )
        gathered = (gathered / totals).astype(jnp.bfloat16)
        values = [
            jnp.dot(
                gathered[place_of * row_count : (place_of + 1) * row_count],
                value_up[:, (head + place_of) * size : (head + place_of + 1) * size],
                preferred_element_type=jnp.float32,
            ).astype(jnp.bfloat16)
            for place_of in range(count)
        ]
        with jax.named_scope(f"att_done{index}"):
            attended[:, head * size : (head + count) * size] = jnp.concatenate(values, axis=1)
        if index == len(groups) - 1:
            relay(pairs, 1)

    for copy in out_copies:
        with jax.named_scope('outcopy'):
            copy.wait()
    share = jnp.dot(
        attended_small[...], out_small_held[...], preferred_element_type=jnp.float32
    ) + jnp.dot(attended_large[...], out_large_held[...], preferred_element_type=jnp.float32)
    mixed_part[...] = share.reshape(tp_count, own_rows, model)

    def mixed_copy(other_tp):
        tp_to = flip(tp_index, other_tp)
        return remote(
            mixed_other.at[0, other_tp - 1],
            mixed_other.at[1, other_tp - 1],
            mixed_send.at[1, other_tp - 1],
            mixed_recv.at[1, other_tp - 1],
            place(far_index, near_index, tp_to),
        )

    for other_tp in range(1, tp_count):
        mixed_other[0, other_tp - 1] = mixed_part[flip(tp_index, other_tp)].astype(jnp.bfloat16)
        mixed_copy(other_tp).start()
    mixed = mixed_part[tp_index]
    for other_tp in range(1, tp_count):
        with jax.named_scope('wait_mixed'):
            mixed_copy(other_tp).wait_recv()
        mixed = mixed + mixed_other[1, other_tp - 1].astype(jnp.float32)
    mixed = mixed.astype(jnp.bfloat16).astype(jnp.float32)
    stream[...] = (residual[...].astype(jnp.float32) + mixed).astype(jnp.bfloat16)
    as_float = stream[...].astype(jnp.float32)
    spread = lax.rsqrt(jnp.mean(as_float * as_float, axis=1, keepdims=True) + norm_eps)
    normed = as_float * spread * gain[...].astype(jnp.float32).reshape(1, model)
    with jax.named_scope('normed'):
        rows_all[far_index, tp_index] = normed.astype(jnp.bfloat16)

    far_bits = far.bit_length() - 1
    pieces = 2 if model % (2 * LANES) == 0 else 1
    piece_width = model // pieces

    def rows_sends():
        sends = []
        for role in range(far):
            low = min([b for b in range(far_bits) if role >> b & 1], default=far_bits)
            sends += [(role, bit) for bit in reversed(range(low))]
        return sends

    def rows_part(role, piece):
        span = pl.ds(piece * piece_width, piece_width)
        return rows_all.at[flip(far_index, role), tp_index, :, span]

    def rows_copy(role, bit, piece):
        return remote(
            rows_part(role, piece),
            rows_part(role, piece),
            rows_send.at[0],
            rows_recv.at[role | 1 << bit, piece],
            place(flip(far_index, 1 << bit), near_index, tp_index),
        )

    def pair_copy(role, other_tp, piece):
        return remote(
            rows_part(role, piece),
            rows_part(role, piece),
            pair_send.at[other_tp - 1],
            pair_recv.at[other_tp - 1],
            place(far_index, near_index, flip(tp_index, other_tp)),
        )

    def rows_pass(role, piece):
        for sender, bit in rows_sends():
            if sender == role:
                rows_copy(role, bit, piece).start()
        for other_tp in range(1, tp_count):
            pair_copy(role, other_tp, piece).start()

    def rows_take(role):
        for piece in range(pieces):
            with jax.named_scope(f"wait_rows{role}_{piece}"):
                remote(
                    rows_part(role, piece),
                    rows_part(role, piece),
                    copy_sem.at[0],
                    rows_recv.at[role, piece],
                    place(flip(far_index, 1), near_index, tp_index),
                ).wait_recv()
            rows_pass(role, piece)

    for piece in range(pieces):
        rows_pass(0, piece)
    for step in reversed(range(3, far)):
        start_far(2, step)
    relayed = sorted({role for role, _ in rows_sends() if role}, reverse=True)
    leaves = [role for role in range(1, far) if role not in relayed]
    for step in range(2, far):
        take(pairs, step, 0)
    relay((2,), 0)
    for step in range(2, far // 2 + 1):
        relay(pairs, step)
    for role in relayed:
        rows_take(role)
    if far > 2:
        start_far(2, 2)
    for step in range(far // 2 + 1, far):
        relay(pairs, step)
    take((2,), 1, 0)
    for role in leaves:
        rows_take(role)
    for step in reversed(range(3, far)):
        take((2,), step, 0)
    for other_tp in range(1, tp_count):
        with jax.named_scope("wait_pair"):
            pltpu.make_async_copy(
                rows_all.at[:, 0], rows_all.at[:, 0], pair_recv.at[other_tp - 1]
            ).wait()

    tile = 2 * LANES if width % (2 * LANES) == 0 else LANES
    for step in range(far):
        take_group(pairs, step)
        start = aligned(flip(far_index, step), chunk)
        rows = rows_all[:, :, :, pl.ds(start, chunk)].reshape(row_total, chunk)
        for first in range(0, width, tile):
            span = pl.ds(first, tile)
            for weight, total in ((gate_all, gate_sum), (up_all, up_sum)):
                product = jnp.dot(
                    rows, weight[pl.ds(start, chunk), span], preferred_element_type=jnp.float32
                )
                total[:, span] = product if step == 0 else total[:, span] + product
    for first in range(0, width, LANES):
        span = pl.ds(first, LANES)
        value = gate_sum[:, span]
        value = (value / (1.0 + jnp.exp(-value)) * up_sum[:, span]).astype(hidden.dtype)
        if first >= (wide - 1) * LANES and tiles % far:
            value = jnp.where(own_count == wide, value, jnp.zeros_like(value))
        hidden[:, span] = value

    half = chunk // 2

    def columns_of(step, side):
        top = near // 2
        return flip(far_index, step) * 2 + lax.rem(lax.div(near_index, top) + side, 2)

    def columns_of_far(step, side, apart):
        top = near // 2
        group = flip(flip(far_index, apart), step)
        return group * 2 + lax.rem(lax.div(near_index, top) + side, 2)

    def part_copy(step, side, other_tp):
        tp_to = flip(tp_index, other_tp)
        return remote(
            part.at[step * 2 + side, :, tp_to],
            other.at[step * 2 + side, other_tp - 1],
            part_send.at[other_tp - 1],
            part_recv.at[step * 2 + side, other_tp - 1],
            place(far_index, near_index, tp_to),
        )

    def sum_copy(step, side, apart):
        far_to = flip(far_index, apart)
        return remote(
            summed.at[step * 2 + side, far_to],
            arrived.at[apart - 1, columns_of(step, side)],
            sum_send.at[0],
            sum_recv.at[step * 2 + side],
            place(far_to, near_index, tp_index),
        )

    def finish(step, side):
        total = part[step * 2 + side, :, tp_index].astype(jnp.float32)
        for other_tp in range(1, tp_count):
            with jax.named_scope(f"wait_part{step}_{side}"):
                part_copy(step, side, other_tp).wait_recv()
            total = total + other[step * 2 + side, other_tp - 1].astype(jnp.float32)
        summed[step * 2 + side] = total.astype(summed.dtype)
        for apart in range(1, far):
            sum_copy(step, side, apart).start()
        own_sum[columns_of(step, side)] = summed[step * 2 + side, far_index].astype(jnp.float32)

    def down_part(step, side):
        for role in range(side * near // 2, (side + 1) * near // 2):
            take((2,), step, role)
        start = aligned(columns_of(step, side), half)
        product = lax.dot_general(
            hidden[...],
            down_all[pl.ds(start, half), :],
            (((1,), (1,)), ((), ())),
            preferred_element_type=jnp.float32,
        )
        with jax.named_scope(f"downdot{step}_{side}"):
            part[step * 2 + side] = product.reshape(far, tp_count, own_rows, half).astype(part.dtype)
        for other_tp in range(1, tp_count):
            part_copy(step, side, other_tp).start()

    if far > 2:
        take((2,), 2, 0)
    order = [0, 1] + list(reversed(range(2, far)))
    parts = [(step, side) for step in order for side in range(2)]
    for number, (step, side) in enumerate(parts):
        down_part(step, side)
        if number + 1 < far:
            relay((2,), order[number + 1])
        if number:
            finish(*parts[number - 1])
    finish(*parts[-1])

    def await_bytes(ref, semaphore):
        pltpu.make_async_copy(ref, ref, semaphore).wait()

    await_bytes(keys_all.at[0, pl.ds(0, far * near - 1)], keys_send.at[0])
    for other_tp in range(1, tp_count):
        key_pair(other_tp).wait_send()
        mixed_copy(other_tp).wait_send()
        await_bytes(rows_all.at[:, 0], pair_send.at[other_tp - 1])
        await_bytes(other.at[:, 0], part_send.at[other_tp - 1])
    for matrix in range(3):

        def await_far(number):
            columns = pl.ds(0, (tiles - number) * LANES)
            await_bytes(inputs[matrix].at[:, columns], far_send.at[matrix])

        def await_near(number):
            rows = pl.ds(0, far * (near - 1) * depth)
            await_bytes(held[matrix].at[rows, pl.ds(0, number * LANES)], near_send.at[matrix])

        if tiles % far == 0:
            await_far(wide)
        else:
            for number in (wide - 1, wide):
                pl.when(own_count == number)(functools.partial(await_far, number))
        by_count(own_count, await_near)
    await_bytes(rows_all.at[pl.ds(0, far - 1), 0], rows_send.at[0])
    for step, side in parts:
        with jax.named_scope(f"wait_sum{step}_{side}"):
            await_bytes(arrived.at[:, 0], sum_recv.at[step * 2 + side])
        for apart in range(1, far):
            columns = columns_of_far(step, side, apart)
            own_sum[columns] = own_sum[columns] + arrived[apart - 1, columns].astype(jnp.float32)
    for place_of in range(2 * far):
        span = pl.ds(place_of * half, half)
        channel = own_sum[place_of].astype(jnp.bfloat16).astype(jnp.float32)
        out[:, span] = (stream[:, span].astype(jnp.float32) + 0.5 * channel).astype(out.dtype)

    await_bytes(summed.at[:, pl.ds(0, far - 1)], sum_send.at[0])


def shards(
    residual,
    query_small,
    query_large,
    latent,
    rope_key,
    key_up_small,
    value_up_small,
    key_up_large,
    value_up_large,
    out_small,
    out_large,
    norm_gain,
    gate_weight,
    up_weight,
    down_weight,
):
    sp_count = lax.axis_size("sp")
    tp_count = lax.axis_size("tp")
    far = 1
    while far * far < sp_count:
        far *= 2
    near = sp_count // far
    spare = -gate_weight.shape[1] % LANES
    if spare:
        gate_weight, up_weight, down_weight = (
            jnp.pad(weight, ((0, 0), (0, spare))) for weight in (gate_weight, up_weight, down_weight)
        )
    own_rows, model = residual.shape
    row_count, latent_width = latent.shape
    depth, units = gate_weight.shape
    tiles = units // LANES
    wide = -(-tiles // far)
    width = wide * LANES
    chunk = near * depth
    row_total = far * tp_count * own_rows
    key_total = sp_count * row_count
    key_width = -(-(latent_width + ROPE) // LANES) * LANES
    small, large = out_small.shape[0], out_large.shape[0]
    heads = small // HEAD_SMALL + large // HEAD_LARGE
    rates = 1.0 / rope_base ** (np.arange(0, ROPE, 2, dtype=np.float32) / ROPE)
    small_operands = (
        residual,
        query_small,
        query_large,
        latent,
        rope_key.T,
        jnp.asarray(rates[None, :], jnp.float32),
        key_up_small,
        value_up_small,
        key_up_large,
        value_up_large,
        norm_gain,
    )
    plan = (far, near, tp_count, depth, tiles, wide, width)
    bf16, f32 = jnp.bfloat16, jnp.float32
    others = max(tp_count - 1, 1)
    slot_count = far * near + 2 * far * (near // 2) + far
    dma = pltpu.SemaphoreType.DMA
    vmem = pl.BlockSpec(memory_space=pltpu.VMEM)
    anywhere = pl.BlockSpec(memory_space=pl.ANY)
    return pl.pallas_call(
        functools.partial(mixer, plan),
        out_shape=jax.ShapeDtypeStruct((own_rows, model), bf16),
        in_specs=[anywhere] * 16,
        out_specs=vmem,
        scratch_shapes=[pltpu.VMEM(value.shape, value.dtype) for value in small_operands]
        + [
            pltpu.VMEM((tp_count, own_rows, key_width), bf16),
            pltpu.VMEM((tp_count, sp_count, own_rows, key_width), bf16),
            pltpu.VMEM((heads * row_count, key_width), bf16),
            pltpu.VMEM((row_count, key_total), f32),
            pltpu.VMEM((row_count, small), bf16),
            pltpu.VMEM((row_count, large), bf16),
            pltpu.VMEM(out_small.shape, bf16),
            pltpu.VMEM(out_large.shape, bf16),
            pltpu.VMEM((tp_count, own_rows, model), f32),
            pltpu.VMEM((2, others, own_rows, model), bf16),
            pltpu.VMEM((own_rows, model), bf16),
            pltpu.VMEM((model, width), bf16),
            pltpu.VMEM((model, width), bf16),
            pltpu.VMEM((model, width), bf16),
            pltpu.VMEM((far, tp_count, own_rows, model), bf16),
            pltpu.VMEM((row_total, width), f32),
            pltpu.VMEM((row_total, width), f32),
            pltpu.VMEM((row_total, width), bf16),
            pltpu.VMEM((2 * far, far, tp_count, own_rows, chunk // 2), bf16),
            pltpu.VMEM((2 * far, others, far, own_rows, chunk // 2), bf16),
            pltpu.VMEM((2 * far, far, own_rows, chunk // 2), bf16),
            pltpu.VMEM((far - 1, 2 * far, own_rows, chunk // 2), bf16),
            pltpu.VMEM((2 * far, own_rows, chunk // 2), f32),
            dma((3,)),
            dma((2,)),
            dma((len(small_operands),)),
            dma((3,)),
            dma((3,)),
            dma((slot_count,)),
            dma((1,)),
            dma((far, max(near // 2, 2))),
            dma((2, others)),
            dma((2, others)),
            dma((1,)),
            dma((far, 2)),
            dma((others,)),
            dma((others,)),
            dma((others,)),
            dma((2 * far, others)),
            dma((1,)),
            dma((2 * far,)),
        ],
        compiler_params=pltpu.CompilerParams(
            collective_id=0, has_side_effects=True, vmem_limit_bytes=58 * 1024 * 1024
        ),
    )(
        *small_operands,
        out_small,
        out_large,
        gate_weight,
        up_weight,
        down_weight,
    )


def solution(mesh):
    placed = (
        P(("sp", "tp"), None),
        P("sp", "tp"),
        P("sp", "tp"),
        P("sp", None),
        P("sp", None),
        P(None, "tp"),
        P(None, "tp"),
        P(None, "tp"),
        P(None, "tp"),
        P("tp", None),
        P("tp", None),
        P(),
        P("sp", "tp"),
        P("sp", "tp"),
        P("sp", "tp"),
    )
    return jax.shard_map(
        shards, mesh=mesh, in_specs=placed, out_specs=P(("sp", "tp"), None), check_vma=False
    )
```

```python
import functools
import math

import jax
import jax.numpy as jnp
import numpy as np
from jax import lax
from jax.experimental import pallas as pl
from jax.experimental.pallas import tpu as pltpu
from jax.sharding import PartitionSpec as P

MESH = pl.DeviceIdType.MESH
HEAD_SMALL = 64
HEAD_LARGE = 128
ROPE = 32
LANES = 128


big_negative = -1e30
rope_base = 500000.0
norm_eps = 1e-06


def flip(index, mask):
    bit = 1
    while bit <= mask:
        if mask & bit:
            index = index + bit * (1 - 2 * lax.rem(lax.div(index, bit), 2))
        bit *= 2
    return index


def aligned(index, size):
    return pl.multiple_of(index * size, size)


def mixer(
    plan,
    residual_in,
    query_small_in,
    query_large_in,
    latent_in,
    rope_key_in,
    turn_rates_in,
    key_up_small_in,
    value_up_small_in,
    key_up_large_in,
    value_up_large_in,
    gain_in,
    out_small,
    out_large,
    gate,
    up,
    down,
    out,
    residual,
    query_small,
    query_large,
    latent,
    rope_key,
    turn_rates,
    key_up_small,
    value_up_small,
    key_up_large,
    value_up_large,
    gain,
    keys_own,
    keys_all,
    queries,
    bias,
    attended_small,
    attended_large,
    out_small_held,
    out_large_held,
    mixed_part,
    mixed_other,
    stream,
    gate_all,
    up_all,
    down_all,
    rows_all,
    gate_sum,
    up_sum,
    hidden,
    part,
    other,
    summed,
    arrived,
    own_sum,
    copy_sem,
    out_sem,
    small_sem,
    far_send,
    near_send,
    weight_recv,
    keys_send,
    keys_recv,
    mixed_send,
    mixed_recv,
    rows_send,
    rows_recv,
    pair_send,
    pair_recv,
    part_send,
    part_recv,
    sum_send,
    sum_recv,
):
    far, near, tp_count, depth, tiles, wide, width = plan
    own_rows, model = residual.shape
    row_count, latent_width = latent.shape
    near_bits = near.bit_length() - 1
    chunk = near * depth
    row_total = far * tp_count * own_rows
    sp_index = lax.axis_index("sp")
    tp_index = lax.axis_index("tp")
    far_index = lax.div(sp_index, near)
    near_index = lax.rem(sp_index, near)

    def place(far_to, near_to, tp_to):
        return {"sp": far_to * near + near_to, "tp": tp_to}

    def first_tile(far_to):
        return lax.div(far_to * tiles + lax.rem(tp_index, 2) * (far - 1), far)

    def tile_count(far_to):
        return first_tile(far_to + 1) - first_tile(far_to)

    def by_count(count, act):
        if tiles % far == 0:
            act(wide)
            return
        for number in (wide - 1, wide):
            if number:
                pl.when(count == number)(functools.partial(act, number))

    inputs = (gate, up, down)
    held = (gate_all, up_all, down_all)
    own_count = tile_count(far_index)

    def source(matrix, far_to, number):
        start = aligned(first_tile(far_to), LANES)
        return inputs[matrix].at[:, pl.ds(start, number * LANES)]

    def block(matrix, far_from, near_from, number):
        start = aligned(far_from * near + near_from, depth)
        return held[matrix].at[pl.ds(start, depth), pl.ds(0, number * LANES)]

    def remote(src, dst, send, recv, device):
        return pltpu.make_async_remote_copy(
            src_ref=src,
            dst_ref=dst,
            send_sem=send,
            recv_sem=recv,
            device_id=device,
            device_id_type=MESH,
        )

    def own_copy(matrix, number):
        return pltpu.make_async_copy(
            source(matrix, far_index, number),
            block(matrix, far_index, near_index, number),
            copy_sem.at[matrix],
        )

    def far_copy(matrix, step, number):
        far_to = flip(far_index, step)
        return remote(
            source(matrix, far_to, number),
            block(matrix, far_index, near_index, number),
            far_send.at[matrix],
            weight_recv.at[slot(matrix, step, 0)],
            place(far_to, near_index, tp_index),
        )

    def near_order(step):
        return [(step + number) % near_bits for number in range(near_bits)]

    def near_sends(step):
        order = near_order(step)
        sends = []
        for role in range(near):
            reached = max([order.index(b) for b in range(near_bits) if role >> b & 1], default=-1)
            for bit in order[reached + 1 :]:
                sends.append((role, bit))
        return sends

    slots = {}

    def is_leaf(matrix, step, role):
        return role > 0 and all(sender != role for sender, _ in near_sends(step + matrix))

    def slot(matrix, step, role):
        shared = matrix < 2 and is_leaf(matrix, step, role)
        return slots.setdefault(("leaf", step) if shared else (matrix, step, role), len(slots))

    def near_copy(matrix, step, role, bit, number):
        far_from = flip(far_index, step)
        near_from = flip(near_index, role)
        target = block(matrix, far_from, near_from, number)
        direct = step == 0 and role == 0
        return remote(
            source(matrix, far_index, number) if direct else target,
            target,
            near_send.at[matrix],
            weight_recv.at[slot(matrix, step, role | 1 << bit)],
            place(far_index, flip(near_index, 1 << bit), tp_index),
        )

    def start_far(matrix, step):
        by_count(
            tile_count(flip(far_index, step)),
            lambda number: far_copy(matrix, step, number).start(),
        )

    def forward(matrix, step, role):
        def act(number):
            for sender, bit in near_sends(step + matrix):
                if sender == role:
                    near_copy(matrix, step, role, bit, number).start()

        by_count(own_count, act)

    def await_block(matrix, step, role):
        with jax.named_scope(f"wait_m{matrix}_s{step}_r{role}"):
            await_block_(matrix, step, role)

    def await_block_(matrix, step, role):
        def act(number):
            if role == 0 and step == 0:
                own_copy(matrix, number).wait()
            else:
                far_from, near_from = flip(far_index, step), flip(near_index, role)
                target = block(matrix, far_from, near_from, number)
                remote(
                    target,
                    target,
                    copy_sem.at[matrix],
                    weight_recv.at[slot(matrix, step, role)],
                    place(far_index, flip(near_index, 1), tp_index),
                ).wait_recv()

        by_count(own_count, act)

    def relay_roles(step):
        return sorted({role for role, _ in near_sends(step) if role})

    done = set()

    def take(matrices, step, role):
        for matrix in matrices:
            if (matrix, step, role) not in done:
                done.add((matrix, step, role))
                await_block(matrix, step, role)
                if not (step == 0 and role == 0):
                    forward(matrix, step, role)

    def relay(matrices, step):
        for matrix in matrices:
            for role in relay_roles(step + matrix):
                take((matrix,), step, role)

    def take_group(matrices, step):
        leaves_of = [
            (matrix, role)
            for matrix in matrices
            for role in range(near)
            if is_leaf(matrix, step, role)
        ]
        for matrix in matrices:
            for role in range(near):
                if (matrix, role) not in leaves_of:
                    take((matrix,), step, role)

        def act(number):
            rows = gate_all.at[pl.ds(0, len(leaves_of) * depth), pl.ds(0, number * LANES)]
            pltpu.make_async_copy(rows, rows, weight_recv.at[slot(*shared)]).wait()

        shared = (leaves_of[0][0], step, leaves_of[0][1])
        with jax.named_scope(f"wait_leaves_s{step}"):
            by_count(own_count, act)

    barrier = pltpu.get_barrier_semaphore()
    peers = [place(flip(far_index, step), near_index, tp_index) for step in range(1, far)]
    peers += [place(far_index, flip(near_index, 1 << b), tp_index) for b in range(near_bits)]
    peers += [place(far_index, near_index, flip(tp_index, j)) for j in range(1, tp_count)]
    for peer in peers:
        pl.semaphore_signal(barrier, inc=1, device_id=peer, device_id_type=MESH)
    loads = [
        pltpu.make_async_copy(source_ref, held_ref, small_sem.at[place_of])
        for place_of, (source_ref, held_ref) in enumerate(
            (
                (residual_in, residual),
                (query_small_in, query_small),
                (query_large_in, query_large),
                (latent_in, latent),
                (rope_key_in, rope_key),
                (turn_rates_in, turn_rates),
                (key_up_small_in, key_up_small),
                (value_up_small_in, value_up_small),
                (key_up_large_in, key_up_large),
                (value_up_large_in, value_up_large),
                (gain_in, gain),
            )
        )
    ]
    first_loads = (3, 4, 5)
    for number in first_loads:
        loads[number].start()
    for number, load in enumerate(loads):
        if number not in first_loads:
            load.start()
    for number in first_loads:
        loads[number].wait()

    rates = turn_rates[...]

    def turning(first, count):
        rows = first + lax.broadcasted_iota(jnp.int32, (count, 1), 0)
        angles = rows.astype(jnp.float32) * rates
        cosine, sine = jnp.cos(angles), jnp.sin(angles)
        return (
            jnp.concatenate([cosine, cosine], axis=1),
            jnp.concatenate([-sine, sine], axis=1),
        )

    def turned(vectors, table):
        half = vectors.shape[1] // 2
        vectors = vectors.astype(jnp.float32)
        swapped = jnp.concatenate([vectors[:, half:], vectors[:, :half]], axis=1)
        return vectors * table[0] + swapped * table[1]

    first_row = sp_index * row_count
    query_table = turning(first_row, row_count)
    key_turn = turned(rope_key[...].T, query_table).astype(jnp.bfloat16)
    key_pad = jnp.zeros((row_count, keys_all.shape[3] - latent_width - ROPE), jnp.bfloat16)
    own_keys = jnp.concatenate([latent[...], key_turn, key_pad], axis=1)
    keys_own[...] = own_keys.reshape(tp_count, own_rows, keys_all.shape[3])
    keys_all[tp_index, sp_index] = keys_own[tp_index]

    if tiles % far:
        spare = pl.ds((wide - 1) * LANES, LANES)

        @pl.when(own_count < wide)
        def _():
            gate_all[:, spare] = jnp.zeros((far * chunk, LANES), gate_all.dtype)
            up_all[:, spare] = jnp.zeros((far * chunk, LANES), up_all.dtype)
            down_all[:, spare] = jnp.zeros((far * chunk, LANES), down_all.dtype)

    with jax.named_scope('barrier'):
        pl.semaphore_wait(barrier, len(peers))

    def key_block(step, role):
        return keys_all.at[tp_index, flip(far_index, step) * near + flip(near_index, role)]

    def key_far(step):
        return remote(
            key_block(0, 0),
            key_block(0, 0),
            keys_send.at[0],
            keys_recv.at[step, 0],
            place(flip(far_index, step), near_index, tp_index),
        )

    def key_slot(step, role):
        if role == 0:
            return step, 0
        return (step, 1 + relay_roles(step).index(role)) if role in relay_roles(step) else (0, 0)

    def key_near(step, role, bit):
        return remote(
            key_block(step, role),
            key_block(step, role),
            keys_send.at[0],
            keys_recv.at[key_slot(step, role | 1 << bit)],
            place(far_index, flip(near_index, 1 << bit), tp_index),
        )

    def key_forward(step, role):
        for sender, bit in near_sends(step):
            if sender == role:
                key_near(step, role, bit).start()

    def key_take(step, role):
      with jax.named_scope(f"wait_key_s{step}_r{role}"):
        remote(
            key_block(step, role),
            key_block(step, role),
            copy_sem.at[0],
            keys_recv.at[key_slot(step, role)],
            place(far_index, flip(near_index, 1), tp_index),
        ).wait_recv()
        key_forward(step, role)

    def key_pair(other_tp):
        return remote(
            keys_all.at[tp_index],
            keys_all.at[tp_index],
            mixed_send.at[0, other_tp - 1],
            mixed_recv.at[0, other_tp - 1],
            place(far_index, near_index, flip(tp_index, other_tp)),
        )

    pairs = (0, 1)
    for step in range(1, far):
        key_far(step).start()
    key_forward(0, 0)
    for matrix in pairs:
        forward(matrix, 0, 0)
    for matrix in pairs:
        start_far(matrix, 1)
    inner = lax.rem(lax.div(far_index, max(far // 2, 1)) + lax.div(far_index, max(far // 4, 1)), 2)

    def start_rest(steps):
        for matrix in pairs:
            for step in steps:
                start_far(matrix, step)

    pl.when(inner == 0)(lambda: start_rest(range(2, far)))
    pl.when(inner == 1)(lambda: start_rest(range(far - 1, 1, -1)))
    start_far(2, 1)
    out_copies = [
        pltpu.make_async_copy(out_small, out_small_held, out_sem.at[0]),
        pltpu.make_async_copy(out_large, out_large_held, out_sem.at[1]),
    ]
    for copy in out_copies:
        copy.start()
    for matrix in range(3):
        by_count(own_count, lambda number: own_copy(matrix, number).start())

    for number, load in enumerate(loads):
        if number not in first_loads:
            load.wait()

    groups = []
    lifted = 0
    for query, key_up, value_up, attended, size in (
        (query_small, key_up_small, value_up_small, attended_small, HEAD_SMALL),
        (query_large, key_up_large, value_up_large, attended_large, HEAD_LARGE),
    ):
        span_width = size + ROPE
        heads = query.shape[1] // span_width
        scale = float(span_width) ** -0.5 * math.log2(math.e)
        pad = jnp.zeros((row_count, keys_all.shape[3] - latent_width - ROPE), jnp.bfloat16)
        for head in range(heads):
            vector = query[:, head * span_width : (head + 1) * span_width]
            content = lax.dot_general(
                vector[:, :size],
                key_up[:, head * size : (head + 1) * size],
                (((1,), (1,)), ((), ())),
                preferred_element_type=jnp.float32,
            )
            rotary = turned(vector[:, size:], query_table)
            queries[lifted * row_count : (lifted + 1) * row_count, :] = jnp.concatenate(
                [(content * scale).astype(jnp.bfloat16), (rotary * scale).astype(jnp.bfloat16), pad],
                axis=1,
            )
            if head % 2 == 0:
                groups.append((lifted, head, min(2, heads - head), size, value_up, attended))
            lifted += 1
    key_total = tp_count * far * near * own_rows
    number = lax.broadcasted_iota(jnp.int32, (1, key_total), 1)
    key_tp = lax.div(number, far * near * own_rows)
    key_rest = lax.rem(number, far * near * own_rows)
    key_pos = (
        lax.div(key_rest, own_rows) * row_count + key_tp * own_rows + lax.rem(key_rest, own_rows)
    )
    query_pos = first_row + lax.broadcasted_iota(jnp.int32, (row_count, 1), 0)
    bias[...] = jnp.where(key_pos <= query_pos, 0.0, big_negative)

    for step in range(1, far):
        key_take(step, 0)
        for role in relay_roles(step - 1):
            key_take(step - 1, role)
    relay(pairs, 0)
    for role in relay_roles(far - 1):
        key_take(far - 1, role)
    take(pairs, 1, 0)
    forward(2, 0, 0)
    key_leaves = far * near - far - sum(len(relay_roles(step)) for step in range(far))
    leaf_blocks = keys_all.at[0, pl.ds(0, key_leaves)]
    with jax.named_scope("wait_keyleaves"):
        pltpu.make_async_copy(leaf_blocks, leaf_blocks, keys_recv.at[0, 0]).wait()
    for other_tp in range(1, tp_count):
        key_pair(other_tp).start()
    for other_tp in range(1, tp_count):
        with jax.named_scope("wait_keypair"):
            key_pair(other_tp).wait_recv()

    for index, (first_head, head, count, size, value_up, attended) in enumerate(groups):
        rows = pl.ds(first_head * row_count, count * row_count)
        keys = keys_all[...].reshape(key_total, keys_all.shape[3])
        scores = lax.dot_general(
            queries[rows, :], keys, (((1,), (1,)), ((), ())), preferred_element_type=jnp.float32
        )
        masked = scores.reshape(count, row_count, key_total) + bias[...][None]
        masked = masked.reshape(count * row_count, key_total)
        weights = jnp.exp2(masked - jnp.max(masked, axis=1, keepdims=True))
        totals = jnp.sum(weights, axis=1, keepdims=True)
        gathered = jnp.dot(
            weights.astype(jnp.bfloat16),
            keys[:, :latent_width],
            preferred_element_type=jnp.float32,
        )
        gathered = (gathered / totals).astype(jnp.bfloat16)
        values = [
            jnp.dot(
                gathered[place_of * row_count : (place_of + 1) * row_count],
                value_up[:, (head + place_of) * size : (head + place_of + 1) * size],
                preferred_element_type=jnp.float32,
            ).astype(jnp.bfloat16)
            for place_of in range(count)
        ]
        with jax.named_scope(f"att_done{index}"):
            attended[:, head * size : (head + count) * size] = jnp.concatenate(values, axis=1)
        if index == len(groups) - 1:
            relay(pairs, 1)

    for copy in out_copies:
        with jax.named_scope('outcopy'):
            copy.wait()
    share = jnp.dot(
        attended_small[...], out_small_held[...], preferred_element_type=jnp.float32
    ) + jnp.dot(attended_large[...], out_large_held[...], preferred_element_type=jnp.float32)
    mixed_part[...] = share.reshape(tp_count, own_rows, model)

    def mixed_copy(other_tp):
        tp_to = flip(tp_index, other_tp)
        return remote(
            mixed_other.at[0, other_tp - 1],
            mixed_other.at[1, other_tp - 1],
            mixed_send.at[1, other_tp - 1],
            mixed_recv.at[1, other_tp - 1],
            place(far_index, near_index, tp_to),
        )

    for other_tp in range(1, tp_count):
        mixed_other[0, other_tp - 1] = mixed_part[flip(tp_index, other_tp)].astype(jnp.bfloat16)
        mixed_copy(other_tp).start()
    for step in range(2, far):
        take(pairs[:1], step, 0)
    mixed = mixed_part[tp_index]
    for other_tp in range(1, tp_count):
        with jax.named_scope('wait_mixed'):
            mixed_copy(other_tp).wait_recv()
        mixed = mixed + mixed_other[1, other_tp - 1].astype(jnp.float32)
    mixed = mixed.astype(jnp.bfloat16).astype(jnp.float32)
    stream[...] = (residual[...].astype(jnp.float32) + mixed).astype(jnp.bfloat16)
    as_float = stream[...].astype(jnp.float32)
    spread = lax.rsqrt(jnp.mean(as_float * as_float, axis=1, keepdims=True) + norm_eps)
    normed = as_float * spread * gain[...].astype(jnp.float32).reshape(1, model)
    with jax.named_scope('normed'):
        rows_all[far_index, tp_index] = normed.astype(jnp.bfloat16)

    far_bits = far.bit_length() - 1
    pieces = 2 if model % (2 * LANES) == 0 else 1
    piece_width = model // pieces

    def rows_sends():
        sends = []
        for role in range(far):
            low = min([b for b in range(far_bits) if role >> b & 1], default=far_bits)
            sends += [(role, bit) for bit in reversed(range(low))]
        return sends

    def rows_part(role, piece):
        span = pl.ds(piece * piece_width, piece_width)
        return rows_all.at[flip(far_index, role), tp_index, :, span]

    def rows_copy(role, bit, piece):
        return remote(
            rows_part(role, piece),
            rows_part(role, piece),
            rows_send.at[0],
            rows_recv.at[role | 1 << bit, piece],
            place(flip(far_index, 1 << bit), near_index, tp_index),
        )

    def pair_copy(role, other_tp, piece):
        return remote(
            rows_part(role, piece),
            rows_part(role, piece),
            pair_send.at[other_tp - 1],
            pair_recv.at[other_tp - 1],
            place(far_index, near_index, flip(tp_index, other_tp)),
        )

    def rows_pass(role, piece):
        for sender, bit in rows_sends():
            if sender == role:
                rows_copy(role, bit, piece).start()
        for other_tp in range(1, tp_count):
            pair_copy(role, other_tp, piece).start()

    def rows_take(role):
        for piece in range(pieces):
            with jax.named_scope(f"wait_rows{role}_{piece}"):
                remote(
                    rows_part(role, piece),
                    rows_part(role, piece),
                    copy_sem.at[0],
                    rows_recv.at[role, piece],
                    place(flip(far_index, 1), near_index, tp_index),
                ).wait_recv()
            rows_pass(role, piece)

    for piece in range(pieces):
        rows_pass(0, piece)
    for step in reversed(range(3, far)):
        start_far(2, step)
    relayed = sorted({role for role, _ in rows_sends() if role}, reverse=True)
    leaves = [role for role in range(1, far) if role not in relayed]
    for step in range(2, far):
        take(pairs[1:], step, 0)
    relay((2,), 0)
    for step in range(2, far):
        relay(pairs[:1], step)
    for role in relayed:
        rows_take(role)
    if far > 2:
        start_far(2, 2)
    for step in range(2, far):
        relay(pairs[1:], step)
    take((2,), 1, 0)
    for role in leaves:
        rows_take(role)
    for step in reversed(range(3, far)):
        take((2,), step, 0)
    for other_tp in range(1, tp_count):
        with jax.named_scope("wait_pair"):
            pltpu.make_async_copy(
                rows_all.at[:, 0], rows_all.at[:, 0], pair_recv.at[other_tp - 1]
            ).wait()

    tile = 2 * LANES if width % (2 * LANES) == 0 else LANES
    for step in range(far):
        take_group(pairs, step)
        start = aligned(flip(far_index, step), chunk)
        rows = rows_all[:, :, :, pl.ds(start, chunk)].reshape(row_total, chunk)
        for first in range(0, width, tile):
            span = pl.ds(first, tile)
            for weight, total in ((gate_all, gate_sum), (up_all, up_sum)):
                product = jnp.dot(
                    rows, weight[pl.ds(start, chunk), span], preferred_element_type=jnp.float32
                )
                total[:, span] = product if step == 0 else total[:, span] + product
    for first in range(0, width, LANES):
        span = pl.ds(first, LANES)
        value = gate_sum[:, span]
        value = (value / (1.0 + jnp.exp(-value)) * up_sum[:, span]).astype(hidden.dtype)
        if first >= (wide - 1) * LANES and tiles % far:
            value = jnp.where(own_count == wide, value, jnp.zeros_like(value))
        hidden[:, span] = value

    half = chunk // 2

    def columns_of(step, side):
        top = near // 2
        return flip(far_index, step) * 2 + lax.rem(lax.div(near_index, top) + side, 2)

    def columns_of_far(step, side, apart):
        top = near // 2
        group = flip(flip(far_index, apart), step)
        return group * 2 + lax.rem(lax.div(near_index, top) + side, 2)

    def part_copy(step, side, other_tp):
        tp_to = flip(tp_index, other_tp)
        return remote(
            part.at[step * 2 + side, :, tp_to],
            other.at[step * 2 + side, other_tp - 1],
            part_send.at[other_tp - 1],
            part_recv.at[step * 2 + side, other_tp - 1],
            place(far_index, near_index, tp_to),
        )

    def sum_copy(step, side, apart):
        far_to = flip(far_index, apart)
        return remote(
            summed.at[step * 2 + side, far_to],
            arrived.at[apart - 1, columns_of(step, side)],
            sum_send.at[0],
            sum_recv.at[step * 2 + side],
            place(far_to, near_index, tp_index),
        )

    def finish(step, side):
        total = part[step * 2 + side, :, tp_index].astype(jnp.float32)
        for other_tp in range(1, tp_count):
            with jax.named_scope(f"wait_part{step}_{side}"):
                part_copy(step, side, other_tp).wait_recv()
            total = total + other[step * 2 + side, other_tp - 1].astype(jnp.float32)
        summed[step * 2 + side] = total.astype(summed.dtype)
        for apart in range(1, far):
            sum_copy(step, side, apart).start()
        own_sum[columns_of(step, side)] = summed[step * 2 + side, far_index].astype(jnp.float32)

    def down_part(step, side):
        for role in range(side * near // 2, (side + 1) * near // 2):
            take((2,), step, role)
        start = aligned(columns_of(step, side), half)
        product = lax.dot_general(
            hidden[...],
            down_all[pl.ds(start, half), :],
            (((1,), (1,)), ((), ())),
            preferred_element_type=jnp.float32,
        )
        with jax.named_scope(f"downdot{step}_{side}"):
            part[step * 2 + side] = product.reshape(far, tp_count, own_rows, half).astype(part.dtype)
        for other_tp in range(1, tp_count):
            part_copy(step, side, other_tp).start()

    if far > 2:
        take((2,), 2, 0)
    order = [0, 1] + list(reversed(range(2, far)))
    parts = [(0, 0), (0, 1)] + [(step, side) for side in range(2) for step in order[1:]]
    down_part(0, 0)
    down_part(0, 1)
    finish(0, 0)
    for number, (step, side) in enumerate(parts[2:], 2):
        if side == 0:
            relay((2,), step)
        finish(*parts[number - 1])
        down_part(step, side)
    finish(*parts[-1])

    def await_bytes(ref, semaphore):
        pltpu.make_async_copy(ref, ref, semaphore).wait()

    await_bytes(keys_all.at[0, pl.ds(0, far * near - 1)], keys_send.at[0])
    for other_tp in range(1, tp_count):
        key_pair(other_tp).wait_send()
        mixed_copy(other_tp).wait_send()
        await_bytes(rows_all.at[:, 0], pair_send.at[other_tp - 1])
        await_bytes(other.at[:, 0], part_send.at[other_tp - 1])
    for matrix in range(3):

        def await_far(number):
            columns = pl.ds(0, (tiles - number) * LANES)
            await_bytes(inputs[matrix].at[:, columns], far_send.at[matrix])

        def await_near(number):
            rows = pl.ds(0, far * (near - 1) * depth)
            await_bytes(held[matrix].at[rows, pl.ds(0, number * LANES)], near_send.at[matrix])

        if tiles % far == 0:
            await_far(wide)
        else:
            for number in (wide - 1, wide):
                pl.when(own_count == number)(functools.partial(await_far, number))
        by_count(own_count, await_near)
    await_bytes(rows_all.at[pl.ds(0, far - 1), 0], rows_send.at[0])
    for step, side in parts:
        with jax.named_scope(f"wait_sum{step}_{side}"):
            await_bytes(arrived.at[:, 0], sum_recv.at[step * 2 + side])
        for apart in range(1, far):
            columns = columns_of_far(step, side, apart)
            own_sum[columns] = own_sum[columns] + arrived[apart - 1, columns].astype(jnp.float32)
    for place_of in range(2 * far):
        span = pl.ds(place_of * half, half)
        channel = own_sum[place_of].astype(jnp.bfloat16).astype(jnp.float32)
        out[:, span] = (stream[:, span].astype(jnp.float32) + 0.5 * channel).astype(out.dtype)

    await_bytes(summed.at[:, pl.ds(0, far - 1)], sum_send.at[0])


def shards(
    residual,
    query_small,
    query_large,
    latent,
    rope_key,
    key_up_small,
    value_up_small,
    key_up_large,
    value_up_large,
    out_small,
    out_large,
    norm_gain,
    gate_weight,
    up_weight,
    down_weight,
):
    sp_count = lax.axis_size("sp")
    tp_count = lax.axis_size("tp")
    far = 1
    while far * far < sp_count:
        far *= 2
    near = sp_count // far
    spare = -gate_weight.shape[1] % LANES
    if spare:
        gate_weight, up_weight, down_weight = (
            jnp.pad(weight, ((0, 0), (0, spare))) for weight in (gate_weight, up_weight, down_weight)
        )
    own_rows, model = residual.shape
    row_count, latent_width = latent.shape
    depth, units = gate_weight.shape
    tiles = units // LANES
    wide = -(-tiles // far)
    width = wide * LANES
    chunk = near * depth
    row_total = far * tp_count * own_rows
    key_total = sp_count * row_count
    key_width = -(-(latent_width + ROPE) // LANES) * LANES
    small, large = out_small.shape[0], out_large.shape[0]
    heads = small // HEAD_SMALL + large // HEAD_LARGE
    rates = 1.0 / rope_base ** (np.arange(0, ROPE, 2, dtype=np.float32) / ROPE)
    small_operands = (
        residual,
        query_small,
        query_large,
        latent,
        rope_key.T,
        jnp.asarray(rates[None, :], jnp.float32),
        key_up_small,
        value_up_small,
        key_up_large,
        value_up_large,
        norm_gain,
    )
    plan = (far, near, tp_count, depth, tiles, wide, width)
    bf16, f32 = jnp.bfloat16, jnp.float32
    others = max(tp_count - 1, 1)
    slot_count = far * near + 2 * far * (near // 2) + far
    dma = pltpu.SemaphoreType.DMA
    vmem = pl.BlockSpec(memory_space=pltpu.VMEM)
    anywhere = pl.BlockSpec(memory_space=pl.ANY)
    return pl.pallas_call(
        functools.partial(mixer, plan),
        out_shape=jax.ShapeDtypeStruct((own_rows, model), bf16),
        in_specs=[anywhere] * 16,
        out_specs=vmem,
        scratch_shapes=[pltpu.VMEM(value.shape, value.dtype) for value in small_operands]
        + [
            pltpu.VMEM((tp_count, own_rows, key_width), bf16),
            pltpu.VMEM((tp_count, sp_count, own_rows, key_width), bf16),
            pltpu.VMEM((heads * row_count, key_width), bf16),
            pltpu.VMEM((row_count, key_total), f32),
            pltpu.VMEM((row_count, small), bf16),
            pltpu.VMEM((row_count, large), bf16),
            pltpu.VMEM(out_small.shape, bf16),
            pltpu.VMEM(out_large.shape, bf16),
            pltpu.VMEM((tp_count, own_rows, model), f32),
            pltpu.VMEM((2, others, own_rows, model), bf16),
            pltpu.VMEM((own_rows, model), bf16),
            pltpu.VMEM((model, width), bf16),
            pltpu.VMEM((model, width), bf16),
            pltpu.VMEM((model, width), bf16),
            pltpu.VMEM((far, tp_count, own_rows, model), bf16),
            pltpu.VMEM((row_total, width), f32),
            pltpu.VMEM((row_total, width), f32),
            pltpu.VMEM((row_total, width), bf16),
            pltpu.VMEM((2 * far, far, tp_count, own_rows, chunk // 2), bf16),
            pltpu.VMEM((2 * far, others, far, own_rows, chunk // 2), bf16),
            pltpu.VMEM((2 * far, far, own_rows, chunk // 2), bf16),
            pltpu.VMEM((far - 1, 2 * far, own_rows, chunk // 2), bf16),
            pltpu.VMEM((2 * far, own_rows, chunk // 2), f32),
            dma((3,)),
            dma((2,)),
            dma((len(small_operands),)),
            dma((3,)),
            dma((3,)),
            dma((slot_count,)),
            dma((1,)),
            dma((far, max(near // 2, 2))),
            dma((2, others)),
            dma((2, others)),
            dma((1,)),
            dma((far, 2)),
            dma((others,)),
            dma((others,)),
            dma((others,)),
            dma((2 * far, others)),
            dma((1,)),
            dma((2 * far,)),
        ],
        compiler_params=pltpu.CompilerParams(
            collective_id=0, has_side_effects=True, vmem_limit_bytes=58 * 1024 * 1024
        ),
    )(
        *small_operands,
        out_small,
        out_large,
        gate_weight,
        up_weight,
        down_weight,
    )


def solution(mesh):
    placed = (
        P(("sp", "tp"), None),
        P("sp", "tp"),
        P("sp", "tp"),
        P("sp", None),
        P("sp", None),
        P(None, "tp"),
        P(None, "tp"),
        P(None, "tp"),
        P(None, "tp"),
        P("tp", None),
        P("tp", None),
        P(),
        P("sp", "tp"),
        P("sp", "tp"),
        P("sp", "tp"),
    )
    return jax.shard_map(
        shards, mesh=mesh, in_specs=placed, out_specs=P(("sp", "tp"), None), check_vma=False
    )
```

```python
import functools
import math

import jax
import jax.numpy as jnp
import numpy as np
from jax import lax
from jax.experimental import pallas as pl
from jax.experimental.pallas import tpu as pltpu
from jax.sharding import PartitionSpec as P

MESH = pl.DeviceIdType.MESH
HEAD_SMALL = 64
HEAD_LARGE = 128
ROPE = 32
LANES = 128


big_negative = -1e30
rope_base = 500000.0
norm_eps = 1e-06


def flip(index, mask):
    bit = 1
    while bit <= mask:
        if mask & bit:
            index = index + bit * (1 - 2 * lax.rem(lax.div(index, bit), 2))
        bit *= 2
    return index


def aligned(index, size):
    return pl.multiple_of(index * size, size)


def mixer(
    plan,
    residual_in,
    query_small_in,
    query_large_in,
    latent_in,
    rope_key_in,
    turn_rates_in,
    key_up_small_in,
    value_up_small_in,
    key_up_large_in,
    value_up_large_in,
    gain_in,
    out_small,
    out_large,
    gate,
    up,
    down,
    out,
    residual,
    query_small,
    query_large,
    latent,
    rope_key,
    turn_rates,
    key_up_small,
    value_up_small,
    key_up_large,
    value_up_large,
    gain,
    keys_own,
    keys_all,
    turned_all,
    queries,
    bias,
    attended_small,
    attended_large,
    out_small_held,
    out_large_held,
    mixed_part,
    mixed_other,
    stream,
    gate_all,
    up_all,
    down_all,
    rows_all,
    gate_sum,
    up_sum,
    hidden,
    part,
    other,
    summed,
    arrived,
    own_sum,
    copy_sem,
    out_sem,
    small_sem,
    far_send,
    near_send,
    weight_recv,
    keys_send,
    keys_recv,
    mixed_send,
    mixed_recv,
    rows_send,
    rows_recv,
    pair_send,
    pair_recv,
    part_send,
    part_recv,
    sum_send,
    sum_recv,
):
    far, near, tp_count, depth, tiles, wide, width = plan
    own_rows, model = residual.shape
    row_count, latent_width = latent.shape
    near_bits = near.bit_length() - 1
    chunk = near * depth
    row_total = far * tp_count * own_rows
    sp_index = lax.axis_index("sp")
    tp_index = lax.axis_index("tp")
    far_index = lax.div(sp_index, near)
    near_index = lax.rem(sp_index, near)

    def place(far_to, near_to, tp_to):
        return {"sp": far_to * near + near_to, "tp": tp_to}

    def first_tile(far_to):
        return lax.div(far_to * tiles + lax.rem(tp_index, 2) * (far - 1), far)

    def tile_count(far_to):
        return first_tile(far_to + 1) - first_tile(far_to)

    def by_count(count, act):
        if tiles % far == 0:
            act(wide)
            return
        for number in (wide - 1, wide):
            if number:
                pl.when(count == number)(functools.partial(act, number))

    inputs = (gate, up, down)
    held = (gate_all, up_all, down_all)
    own_count = tile_count(far_index)

    def source(matrix, far_to, number):
        start = aligned(first_tile(far_to), LANES)
        return inputs[matrix].at[:, pl.ds(start, number * LANES)]

    def block(matrix, far_from, near_from, number):
        start = aligned(far_from * near + near_from, depth)
        return held[matrix].at[pl.ds(start, depth), pl.ds(0, number * LANES)]

    def remote(src, dst, send, recv, device):
        return pltpu.make_async_remote_copy(
            src_ref=src,
            dst_ref=dst,
            send_sem=send,
            recv_sem=recv,
            device_id=device,
            device_id_type=MESH,
        )

    def own_copy(matrix, number):
        return pltpu.make_async_copy(
            source(matrix, far_index, number),
            block(matrix, far_index, near_index, number),
            copy_sem.at[matrix],
        )

    def far_copy(matrix, step, number):
        far_to = flip(far_index, step)
        return remote(
            source(matrix, far_to, number),
            block(matrix, far_index, near_index, number),
            far_send.at[matrix],
            weight_recv.at[slot(matrix, step, 0)],
            place(far_to, near_index, tp_index),
        )

    def near_order(step):
        return [(step + number) % near_bits for number in range(near_bits)]

    def near_sends(step):
        order = near_order(step)
        sends = []
        for role in range(near):
            reached = max([order.index(b) for b in range(near_bits) if role >> b & 1], default=-1)
            for bit in order[reached + 1 :]:
                sends.append((role, bit))
        return sends

    slots = {}

    def is_leaf(matrix, step, role):
        return role > 0 and all(sender != role for sender, _ in near_sends(step + matrix))

    def slot(matrix, step, role):
        shared = matrix < 2 and is_leaf(matrix, step, role)
        return slots.setdefault(("leaf", step) if shared else (matrix, step, role), len(slots))

    def near_copy(matrix, step, role, bit, number):
        far_from = flip(far_index, step)
        near_from = flip(near_index, role)
        target = block(matrix, far_from, near_from, number)
        direct = step == 0 and role == 0
        return remote(
            source(matrix, far_index, number) if direct else target,
            target,
            near_send.at[matrix],
            weight_recv.at[slot(matrix, step, role | 1 << bit)],
            place(far_index, flip(near_index, 1 << bit), tp_index),
        )

    def start_far(matrix, step):
        by_count(
            tile_count(flip(far_index, step)),
            lambda number: far_copy(matrix, step, number).start(),
        )

    def forward(matrix, step, role):
        def act(number):
            for sender, bit in near_sends(step + matrix):
                if sender == role:
                    near_copy(matrix, step, role, bit, number).start()

        by_count(own_count, act)

    def await_block(matrix, step, role):
        with jax.named_scope(f"wait_m{matrix}_s{step}_r{role}"):
            await_block_(matrix, step, role)

    def await_block_(matrix, step, role):
        def act(number):
            if role == 0 and step == 0:
                own_copy(matrix, number).wait()
            else:
                far_from, near_from = flip(far_index, step), flip(near_index, role)
                target = block(matrix, far_from, near_from, number)
                remote(
                    target,
                    target,
                    copy_sem.at[matrix],
                    weight_recv.at[slot(matrix, step, role)],
                    place(far_index, flip(near_index, 1), tp_index),
                ).wait_recv()

        by_count(own_count, act)

    def relay_roles(step):
        return sorted({role for role, _ in near_sends(step) if role})

    done = set()

    def take(matrices, step, role):
        for matrix in matrices:
            if (matrix, step, role) not in done:
                done.add((matrix, step, role))
                await_block(matrix, step, role)
                if not (step == 0 and role == 0):
                    forward(matrix, step, role)

    def relay(matrices, step):
        for matrix in matrices:
            for role in relay_roles(step + matrix):
                take((matrix,), step, role)

    def take_group(matrices, step):
        leaves_of = [
            (matrix, role)
            for matrix in matrices
            for role in range(near)
            if is_leaf(matrix, step, role)
        ]
        for matrix in matrices:
            for role in range(near):
                if (matrix, role) not in leaves_of:
                    take((matrix,), step, role)

        def act(number):
            rows = gate_all.at[pl.ds(0, len(leaves_of) * depth), pl.ds(0, number * LANES)]
            pltpu.make_async_copy(rows, rows, weight_recv.at[slot(*shared)]).wait()

        shared = (leaves_of[0][0], step, leaves_of[0][1])
        with jax.named_scope(f"wait_leaves_s{step}"):
            by_count(own_count, act)

    barrier = pltpu.get_barrier_semaphore()
    peers = [place(flip(far_index, step), near_index, tp_index) for step in range(1, far)]
    peers += [place(far_index, flip(near_index, 1 << b), tp_index) for b in range(near_bits)]
    peers += [place(far_index, near_index, flip(tp_index, j)) for j in range(1, tp_count)]
    for peer in peers:
        pl.semaphore_signal(barrier, inc=1, device_id=peer, device_id_type=MESH)
    loads = [
        pltpu.make_async_copy(source_ref, held_ref, small_sem.at[place_of])
        for place_of, (source_ref, held_ref) in enumerate(
            (
                (residual_in, residual),
                (query_small_in, query_small),
                (query_large_in, query_large),
                (latent_in, latent),
                (rope_key_in, rope_key),
                (turn_rates_in, turn_rates),
                (key_up_small_in, key_up_small),
                (value_up_small_in, value_up_small),
                (key_up_large_in, key_up_large),
                (value_up_large_in, value_up_large),
                (gain_in, gain),
            )
        )
    ]
    first_loads = (3, 4, 5)
    for number in first_loads:
        loads[number].start()
    for number, load in enumerate(loads):
        if number not in first_loads:
            load.start()
    for number in first_loads:
        loads[number].wait()

    rates = turn_rates[...]

    def turning(first, count):
        rows = first + lax.broadcasted_iota(jnp.int32, (count, 1), 0)
        angles = rows.astype(jnp.float32) * rates
        cosine, sine = jnp.cos(angles), jnp.sin(angles)
        return (
            jnp.concatenate([cosine, cosine], axis=1),
            jnp.concatenate([-sine, sine], axis=1),
        )

    def turned(vectors, table):
        half = vectors.shape[1] // 2
        vectors = vectors.astype(jnp.float32)
        swapped = jnp.concatenate([vectors[:, half:], vectors[:, :half]], axis=1)
        return vectors * table[0] + swapped * table[1]

    first_row = sp_index * row_count
    query_table = turning(first_row, row_count)
    key_turn = turned(rope_key[...].T, query_table).astype(jnp.bfloat16)
    fold = latent_width // ROPE
    packed = keys_all.shape[3] == latent_width
    packed_rows = own_rows // fold
    if packed:
        wide_turn = key_turn.astype(jnp.float32)
        for half_of in range(tp_count):
            first = half_of * own_rows
            keys_own[half_of, :own_rows, :] = latent[first : first + own_rows, :]
            pieces_of = [
                wide_turn[first + j * packed_rows : first + (j + 1) * packed_rows]
                for j in range(fold)
            ]
            keys_own[half_of, own_rows:, :] = jnp.concatenate(pieces_of, axis=1).astype(jnp.bfloat16)
    else:
        key_pad = jnp.zeros((row_count, keys_all.shape[3] - latent_width - ROPE), jnp.bfloat16)
        own_keys = jnp.concatenate([latent[...], key_turn, key_pad], axis=1)
        keys_own[...] = own_keys.reshape(tp_count, own_rows, keys_all.shape[3])
    keys_all[tp_index, sp_index] = keys_own[tp_index]

    if tiles % far:
        spare = pl.ds((wide - 1) * LANES, LANES)

        @pl.when(own_count < wide)
        def _():
            gate_all[:, spare] = jnp.zeros((far * chunk, LANES), gate_all.dtype)
            up_all[:, spare] = jnp.zeros((far * chunk, LANES), up_all.dtype)
            down_all[:, spare] = jnp.zeros((far * chunk, LANES), down_all.dtype)

    with jax.named_scope('barrier'):
        pl.semaphore_wait(barrier, len(peers))

    def key_block(step, role):
        return keys_all.at[tp_index, flip(far_index, step) * near + flip(near_index, role)]

    def key_far(step):
        return remote(
            key_block(0, 0),
            key_block(0, 0),
            keys_send.at[0],
            keys_recv.at[step, 0],
            place(flip(far_index, step), near_index, tp_index),
        )

    def key_slot(step, role):
        if role == 0:
            return step, 0
        return (step, 1 + relay_roles(step).index(role)) if role in relay_roles(step) else (0, 0)

    def key_near(step, role, bit):
        return remote(
            key_block(step, role),
            key_block(step, role),
            keys_send.at[0],
            keys_recv.at[key_slot(step, role | 1 << bit)],
            place(far_index, flip(near_index, 1 << bit), tp_index),
        )

    def key_forward(step, role):
        for sender, bit in near_sends(step):
            if sender == role:
                key_near(step, role, bit).start()

    def key_take(step, role):
      with jax.named_scope(f"wait_key_s{step}_r{role}"):
        remote(
            key_block(step, role),
            key_block(step, role),
            copy_sem.at[0],
            keys_recv.at[key_slot(step, role)],
            place(far_index, flip(near_index, 1), tp_index),
        ).wait_recv()
        key_forward(step, role)

    def key_pair(other_tp):
        return remote(
            keys_all.at[tp_index],
            keys_all.at[tp_index],
            mixed_send.at[0, other_tp - 1],
            mixed_recv.at[0, other_tp - 1],
            place(far_index, near_index, flip(tp_index, other_tp)),
        )

    pairs = (0, 1)
    for step in range(1, far):
        key_far(step).start()
    key_forward(0, 0)
    for matrix in pairs:
        forward(matrix, 0, 0)
    for matrix in pairs:
        start_far(matrix, 1)
    inner = lax.rem(lax.div(far_index, max(far // 2, 1)) + lax.div(far_index, max(far // 4, 1)), 2)

    def start_rest(steps):
        for matrix in pairs:
            for step in steps:
                start_far(matrix, step)

    pl.when(inner == 0)(lambda: start_rest(range(2, far)))
    pl.when(inner == 1)(lambda: start_rest(range(far - 1, 1, -1)))
    start_far(2, 1)
    out_copies = [
        pltpu.make_async_copy(out_small, out_small_held, out_sem.at[0]),
        pltpu.make_async_copy(out_large, out_large_held, out_sem.at[1]),
    ]
    for copy in out_copies:
        copy.start()
    for matrix in range(3):
        by_count(own_count, lambda number: own_copy(matrix, number).start())

    for number, load in enumerate(loads):
        if number not in first_loads:
            load.wait()

    groups = []
    lifted = 0
    for query, key_up, value_up, attended, size in (
        (query_small, key_up_small, value_up_small, attended_small, HEAD_SMALL),
        (query_large, key_up_large, value_up_large, attended_large, HEAD_LARGE),
    ):
        span_width = size + ROPE
        heads = query.shape[1] // span_width
        scale = float(span_width) ** -0.5 * math.log2(math.e)
        pad = jnp.zeros((row_count, queries.shape[1] - latent_width - ROPE), jnp.bfloat16)
        for head in range(heads):
            vector = query[:, head * span_width : (head + 1) * span_width]
            content = lax.dot_general(
                vector[:, :size],
                key_up[:, head * size : (head + 1) * size],
                (((1,), (1,)), ((), ())),
                preferred_element_type=jnp.float32,
            )
            rotary = turned(vector[:, size:], query_table)
            queries[lifted * row_count : (lifted + 1) * row_count, :] = jnp.concatenate(
                [(content * scale).astype(jnp.bfloat16), (rotary * scale).astype(jnp.bfloat16), pad],
                axis=1,
            )
            if head % 2 == 0:
                groups.append((lifted, head, min(2, heads - head), size, value_up, attended))
            lifted += 1
    key_total = tp_count * far * near * own_rows
    number = lax.broadcasted_iota(jnp.int32, (1, key_total), 1)
    key_tp = lax.div(number, far * near * own_rows)
    key_rest = lax.rem(number, far * near * own_rows)
    key_pos = (
        lax.div(key_rest, own_rows) * row_count + key_tp * own_rows + lax.rem(key_rest, own_rows)
    )
    query_pos = first_row + lax.broadcasted_iota(jnp.int32, (row_count, 1), 0)
    bias[...] = jnp.where(key_pos <= query_pos, 0.0, big_negative)

    for step in range(1, far):
        key_take(step, 0)
        for role in relay_roles(step - 1):
            key_take(step - 1, role)
    relay(pairs, 0)
    for role in relay_roles(far - 1):
        key_take(far - 1, role)
    take(pairs, 1, 0)
    forward(2, 0, 0)
    key_leaves = far * near - far - sum(len(relay_roles(step)) for step in range(far))
    leaf_blocks = keys_all.at[0, pl.ds(0, key_leaves)]
    with jax.named_scope("wait_keyleaves"):
        pltpu.make_async_copy(leaf_blocks, leaf_blocks, keys_recv.at[0, 0]).wait()
    for other_tp in range(1, tp_count):
        key_pair(other_tp).start()
    for other_tp in range(1, tp_count):
        with jax.named_scope("wait_keypair"):
            key_pair(other_tp).wait_recv()

    if packed:
        for j in range(fold):
            turned_part = keys_all[:, :, own_rows:, j * ROPE : (j + 1) * ROPE].astype(jnp.float32)
            turned_all[:, j * packed_rows : (j + 1) * packed_rows, :] = turned_part.reshape(
                tp_count * far * near, packed_rows, ROPE
            )

    for index, (first_head, head, count, size, value_up, attended) in enumerate(groups):
        rows = pl.ds(first_head * row_count, count * row_count)
        keys = keys_all[:, :, :own_rows, :].reshape(key_total, keys_all.shape[3])
        scores = lax.dot_general(
            queries[rows, : keys.shape[1]],
            keys,
            (((1,), (1,)), ((), ())),
            preferred_element_type=jnp.float32,
        )
        if packed:
            scores = scores + lax.dot_general(
                queries[rows, latent_width : latent_width + ROPE],
                turned_all[...].reshape(key_total, ROPE).astype(jnp.bfloat16),
                (((1,), (1,)), ((), ())),
                preferred_element_type=jnp.float32,
            )
        masked = scores.reshape(count, row_count, key_total) + bias[...][None]
        masked = masked.reshape(count * row_count, key_total)
        weights = jnp.exp2(masked - jnp.max(masked, axis=1, keepdims=True))
        totals = jnp.sum(weights, axis=1, keepdims=True)
        gathered = jnp.dot(
            weights.astype(jnp.bfloat16),
            keys[:, :latent_width],
            preferred_element_type=jnp.float32,
        )
        gathered = (gathered / totals).astype(jnp.bfloat16)
        values = [
            jnp.dot(
                gathered[place_of * row_count : (place_of + 1) * row_count],
                value_up[:, (head + place_of) * size : (head + place_of + 1) * size],
                preferred_element_type=jnp.float32,
            ).astype(jnp.bfloat16)
            for place_of in range(count)
        ]
        with jax.named_scope(f"att_done{index}"):
            attended[:, head * size : (head + count) * size] = jnp.concatenate(values, axis=1)
        if index == len(groups) - 1:
            relay(pairs, 1)

    for copy in out_copies:
        with jax.named_scope('outcopy'):
            copy.wait()
    share = jnp.dot(
        attended_small[...], out_small_held[...], preferred_element_type=jnp.float32
    ) + jnp.dot(attended_large[...], out_large_held[...], preferred_element_type=jnp.float32)
    mixed_part[...] = share.reshape(tp_count, own_rows, model)

    def mixed_copy(other_tp):
        tp_to = flip(tp_index, other_tp)
        return remote(
            mixed_other.at[0, other_tp - 1],
            mixed_other.at[1, other_tp - 1],
            mixed_send.at[1, other_tp - 1],
            mixed_recv.at[1, other_tp - 1],
            place(far_index, near_index, tp_to),
        )

    for other_tp in range(1, tp_count):
        mixed_other[0, other_tp - 1] = mixed_part[flip(tp_index, other_tp)].astype(jnp.bfloat16)
        mixed_copy(other_tp).start()
    for step in range(2, far):
        take(pairs[:1], step, 0)
    mixed = mixed_part[tp_index]
    for other_tp in range(1, tp_count):
        with jax.named_scope('wait_mixed'):
            mixed_copy(other_tp).wait_recv()
        mixed = mixed + mixed_other[1, other_tp - 1].astype(jnp.float32)
    mixed = mixed.astype(jnp.bfloat16).astype(jnp.float32)
    stream[...] = (residual[...].astype(jnp.float32) + mixed).astype(jnp.bfloat16)
    as_float = stream[...].astype(jnp.float32)
    spread = lax.rsqrt(jnp.mean(as_float * as_float, axis=1, keepdims=True) + norm_eps)
    normed = as_float * spread * gain[...].astype(jnp.float32).reshape(1, model)
    with jax.named_scope('normed'):
        rows_all[far_index, tp_index] = normed.astype(jnp.bfloat16)

    far_bits = far.bit_length() - 1
    pieces = 2 if model % (2 * LANES) == 0 else 1
    piece_width = model // pieces

    def rows_sends():
        sends = []
        for role in range(far):
            low = min([b for b in range(far_bits) if role >> b & 1], default=far_bits)
            sends += [(role, bit) for bit in reversed(range(low))]
        return sends

    def rows_part(role, piece):
        span = pl.ds(piece * piece_width, piece_width)
        return rows_all.at[flip(far_index, role), tp_index, :, span]

    def rows_copy(role, bit, piece):
        return remote(
            rows_part(role, piece),
            rows_part(role, piece),
            rows_send.at[0],
            rows_recv.at[role | 1 << bit, piece],
            place(flip(far_index, 1 << bit), near_index, tp_index),
        )

    def pair_copy(role, other_tp, piece):
        return remote(
            rows_part(role, piece),
            rows_part(role, piece),
            pair_send.at[other_tp - 1],
            pair_recv.at[other_tp - 1],
            place(far_index, near_index, flip(tp_index, other_tp)),
        )

    def rows_pass(role, piece):
        for sender, bit in rows_sends():
            if sender == role:
                rows_copy(role, bit, piece).start()
        for other_tp in range(1, tp_count):
            pair_copy(role, other_tp, piece).start()

    def rows_take(role):
        for piece in range(pieces):
            with jax.named_scope(f"wait_rows{role}_{piece}"):
                remote(
                    rows_part(role, piece),
                    rows_part(role, piece),
                    copy_sem.at[0],
                    rows_recv.at[role, piece],
                    place(flip(far_index, 1), near_index, tp_index),
                ).wait_recv()
            rows_pass(role, piece)

    for piece in range(pieces):
        rows_pass(0, piece)
    for step in reversed(range(3, far)):
        start_far(2, step)
    relayed = sorted({role for role, _ in rows_sends() if role}, reverse=True)
    leaves = [role for role in range(1, far) if role not in relayed]
    for step in range(2, far):
        take(pairs[1:], step, 0)
    relay((2,), 0)
    for step in range(2, far):
        relay(pairs[:1], step)
    for role in relayed:
        rows_take(role)
    if far > 2:
        start_far(2, 2)
    for step in range(2, far):
        relay(pairs[1:], step)
    take((2,), 1, 0)
    for role in leaves:
        rows_take(role)
    for step in reversed(range(3, far)):
        take((2,), step, 0)
    for other_tp in range(1, tp_count):
        with jax.named_scope("wait_pair"):
            pltpu.make_async_copy(
                rows_all.at[:, 0], rows_all.at[:, 0], pair_recv.at[other_tp - 1]
            ).wait()

    tile = 2 * LANES if width % (2 * LANES) == 0 else LANES
    for step in range(far):
        take_group(pairs, step)
        start = aligned(flip(far_index, step), chunk)
        rows = rows_all[:, :, :, pl.ds(start, chunk)].reshape(row_total, chunk)
        for first in range(0, width, tile):
            span = pl.ds(first, tile)
            for weight, total in ((gate_all, gate_sum), (up_all, up_sum)):
                product = jnp.dot(
                    rows, weight[pl.ds(start, chunk), span], preferred_element_type=jnp.float32
                )
                total[:, span] = product if step == 0 else total[:, span] + product
    for first in range(0, width, LANES):
        span = pl.ds(first, LANES)
        value = gate_sum[:, span]
        value = (value / (1.0 + jnp.exp(-value)) * up_sum[:, span]).astype(hidden.dtype)
        if first >= (wide - 1) * LANES and tiles % far:
            value = jnp.where(own_count == wide, value, jnp.zeros_like(value))
        hidden[:, span] = value

    half = chunk // 2

    def columns_of(step, side):
        top = near // 2
        return flip(far_index, step) * 2 + lax.rem(lax.div(near_index, top) + side, 2)

    def columns_of_far(step, side, apart):
        top = near // 2
        group = flip(flip(far_index, apart), step)
        return group * 2 + lax.rem(lax.div(near_index, top) + side, 2)

    def part_copy(step, side, other_tp):
        tp_to = flip(tp_index, other_tp)
        return remote(
            part.at[step * 2 + side, :, tp_to],
            other.at[step * 2 + side, other_tp - 1],
            part_send.at[other_tp - 1],
            part_recv.at[step * 2 + side, other_tp - 1],
            place(far_index, near_index, tp_to),
        )

    def sum_copy(step, side, apart):
        far_to = flip(far_index, apart)
        return remote(
            summed.at[step * 2 + side, far_to],
            arrived.at[apart - 1, columns_of(step, side)],
            sum_send.at[0],
            sum_recv.at[step * 2 + side],
            place(far_to, near_index, tp_index),
        )

    def finish(step, side):
        total = part[step * 2 + side, :, tp_index].astype(jnp.float32)
        for other_tp in range(1, tp_count):
            with jax.named_scope(f"wait_part{step}_{side}"):
                part_copy(step, side, other_tp).wait_recv()
            total = total + other[step * 2 + side, other_tp - 1].astype(jnp.float32)
        summed[step * 2 + side] = total.astype(summed.dtype)
        for apart in range(1, far):
            sum_copy(step, side, apart).start()
        own_sum[columns_of(step, side)] = summed[step * 2 + side, far_index].astype(jnp.float32)

    def down_part(step, side):
        for role in range(side * near // 2, (side + 1) * near // 2):
            take((2,), step, role)
        start = aligned(columns_of(step, side), half)
        product = lax.dot_general(
            hidden[...],
            down_all[pl.ds(start, half), :],
            (((1,), (1,)), ((), ())),
            preferred_element_type=jnp.float32,
        )
        with jax.named_scope(f"downdot{step}_{side}"):
            part[step * 2 + side] = product.reshape(far, tp_count, own_rows, half).astype(part.dtype)
        for other_tp in range(1, tp_count):
            part_copy(step, side, other_tp).start()

    if far > 2:
        take((2,), 2, 0)
    order = [0, 1] + list(reversed(range(2, far)))
    parts = [(0, 0), (0, 1)] + [(step, side) for side in range(2) for step in order[1:]]
    down_part(0, 0)
    down_part(0, 1)
    finish(0, 0)
    for number, (step, side) in enumerate(parts[2:], 2):
        if side == 0:
            relay((2,), step)
        finish(*parts[number - 1])
        down_part(step, side)
    finish(*parts[-1])

    def await_bytes(ref, semaphore):
        pltpu.make_async_copy(ref, ref, semaphore).wait()

    await_bytes(keys_all.at[0, pl.ds(0, far * near - 1)], keys_send.at[0])
    for other_tp in range(1, tp_count):
        key_pair(other_tp).wait_send()
        mixed_copy(other_tp).wait_send()
        await_bytes(rows_all.at[:, 0], pair_send.at[other_tp - 1])
        await_bytes(other.at[:, 0], part_send.at[other_tp - 1])
    for matrix in range(3):

        def await_far(number):
            columns = pl.ds(0, (tiles - number) * LANES)
            await_bytes(inputs[matrix].at[:, columns], far_send.at[matrix])

        def await_near(number):
            rows = pl.ds(0, far * (near - 1) * depth)
            await_bytes(held[matrix].at[rows, pl.ds(0, number * LANES)], near_send.at[matrix])

        if tiles % far == 0:
            await_far(wide)
        else:
            for number in (wide - 1, wide):
                pl.when(own_count == number)(functools.partial(await_far, number))
        by_count(own_count, await_near)
    await_bytes(rows_all.at[pl.ds(0, far - 1), 0], rows_send.at[0])
    for step, side in parts:
        with jax.named_scope(f"wait_sum{step}_{side}"):
            await_bytes(arrived.at[:, 0], sum_recv.at[step * 2 + side])
        for apart in range(1, far):
            columns = columns_of_far(step, side, apart)
            own_sum[columns] = own_sum[columns] + arrived[apart - 1, columns].astype(jnp.float32)
    for place_of in range(2 * far):
        span = pl.ds(place_of * half, half)
        channel = own_sum[place_of].astype(jnp.bfloat16).astype(jnp.float32)
        out[:, span] = (stream[:, span].astype(jnp.float32) + 0.5 * channel).astype(out.dtype)

    await_bytes(summed.at[:, pl.ds(0, far - 1)], sum_send.at[0])


def shards(
    residual,
    query_small,
    query_large,
    latent,
    rope_key,
    key_up_small,
    value_up_small,
    key_up_large,
    value_up_large,
    out_small,
    out_large,
    norm_gain,
    gate_weight,
    up_weight,
    down_weight,
):
    sp_count = lax.axis_size("sp")
    tp_count = lax.axis_size("tp")
    far = 1
    while far * far < sp_count:
        far *= 2
    near = sp_count // far
    spare = -gate_weight.shape[1] % LANES
    if spare:
        gate_weight, up_weight, down_weight = (
            jnp.pad(weight, ((0, 0), (0, spare))) for weight in (gate_weight, up_weight, down_weight)
        )
    own_rows, model = residual.shape
    row_count, latent_width = latent.shape
    depth, units = gate_weight.shape
    tiles = units // LANES
    wide = -(-tiles // far)
    width = wide * LANES
    chunk = near * depth
    row_total = far * tp_count * own_rows
    key_total = sp_count * row_count
    key_width = -(-(latent_width + ROPE) // LANES) * LANES
    fold = latent_width // ROPE
    packed = latent_width % LANES == 0 and own_rows % (8 * fold) == 0
    block_rows = own_rows + own_rows // fold if packed else own_rows
    block_width = latent_width if packed else key_width
    small, large = out_small.shape[0], out_large.shape[0]
    heads = small // HEAD_SMALL + large // HEAD_LARGE
    rates = 1.0 / rope_base ** (np.arange(0, ROPE, 2, dtype=np.float32) / ROPE)
    small_operands = (
        residual,
        query_small,
        query_large,
        latent,
        rope_key.T,
        jnp.asarray(rates[None, :], jnp.float32),
        key_up_small,
        value_up_small,
        key_up_large,
        value_up_large,
        norm_gain,
    )
    plan = (far, near, tp_count, depth, tiles, wide, width)
    bf16, f32 = jnp.bfloat16, jnp.float32
    others = max(tp_count - 1, 1)
    slot_count = far * near + 2 * far * (near // 2) + far
    dma = pltpu.SemaphoreType.DMA
    vmem = pl.BlockSpec(memory_space=pltpu.VMEM)
    anywhere = pl.BlockSpec(memory_space=pl.ANY)
    return pl.pallas_call(
        functools.partial(mixer, plan),
        out_shape=jax.ShapeDtypeStruct((own_rows, model), bf16),
        in_specs=[anywhere] * 16,
        out_specs=vmem,
        scratch_shapes=[pltpu.VMEM(value.shape, value.dtype) for value in small_operands]
        + [
            pltpu.VMEM((tp_count, block_rows, block_width), bf16),
            pltpu.VMEM((tp_count, sp_count, block_rows, block_width), bf16),
            pltpu.VMEM((tp_count * sp_count if packed else 1, own_rows, ROPE), f32),
            pltpu.VMEM((heads * row_count, key_width), bf16),
            pltpu.VMEM((row_count, key_total), f32),
            pltpu.VMEM((row_count, small), bf16),
            pltpu.VMEM((row_count, large), bf16),
            pltpu.VMEM(out_small.shape, bf16),
            pltpu.VMEM(out_large.shape, bf16),
            pltpu.VMEM((tp_count, own_rows, model), f32),
            pltpu.VMEM((2, others, own_rows, model), bf16),
            pltpu.VMEM((own_rows, model), bf16),
            pltpu.VMEM((model, width), bf16),
            pltpu.VMEM((model, width), bf16),
            pltpu.VMEM((model, width), bf16),
            pltpu.VMEM((far, tp_count, own_rows, model), bf16),
            pltpu.VMEM((row_total, width), f32),
            pltpu.VMEM((row_total, width), f32),
            pltpu.VMEM((row_total, width), bf16),
            pltpu.VMEM((2 * far, far, tp_count, own_rows, chunk // 2), bf16),
            pltpu.VMEM((2 * far, others, far, own_rows, chunk // 2), bf16),
            pltpu.VMEM((2 * far, far, own_rows, chunk // 2), bf16),
            pltpu.VMEM((far - 1, 2 * far, own_rows, chunk // 2), bf16),
            pltpu.VMEM((2 * far, own_rows, chunk // 2), f32),
            dma((3,)),
            dma((2,)),
            dma((len(small_operands),)),
            dma((3,)),
            dma((3,)),
            dma((slot_count,)),
            dma((1,)),
            dma((far, max(near // 2, 2))),
            dma((2, others)),
            dma((2, others)),
            dma((1,)),
            dma((far, 2)),
            dma((others,)),
            dma((others,)),
            dma((others,)),
            dma((2 * far, others)),
            dma((1,)),
            dma((2 * far,)),
        ],
        compiler_params=pltpu.CompilerParams(
            collective_id=0, has_side_effects=True, vmem_limit_bytes=58 * 1024 * 1024
        ),
    )(
        *small_operands,
        out_small,
        out_large,
        gate_weight,
        up_weight,
        down_weight,
    )


def solution(mesh):
    placed = (
        P(("sp", "tp"), None),
        P("sp", "tp"),
        P("sp", "tp"),
        P("sp", None),
        P("sp", None),
        P(None, "tp"),
        P(None, "tp"),
        P(None, "tp"),
        P(None, "tp"),
        P("tp", None),
        P("tp", None),
        P(),
        P("sp", "tp"),
        P("sp", "tp"),
        P("sp", "tp"),
    )
    return jax.shard_map(
        shards, mesh=mesh, in_specs=placed, out_specs=P(("sp", "tp"), None), check_vma=False
    )
```
